32 devices in a mesh: sp: 8 (over z, y), tp: 4 (over x, core).
Axes of the slice: x: 2, y: 2, z: 4, core: 2. Of those that a mesh axis runs over, the one named last changes fastest.
Arguments:
- glu_value: bfloat16 [4096, 2048], P('sp', 'tp'), may hold values from -640 to 640
- glu_gate: bfloat16 [4096, 2048], P('sp', 'tp'), may hold values from -9 to 9
- conv_kernel: float32 [31, 2048], P(None, 'tp'), may hold values from -1 to 1
- norm_gain: float32 [2048], P('tp'), may hold values from 0.1 to 1.9
- mix_weight: bfloat16 [2048, 2048], P('tp'), may hold values from -0.125 to 0.125
- residual: bfloat16 [4096, 2048], P(('sp', 'tp')), may hold values from -6 to 6
- resid_gain: float32 [2048], replicated, may hold values from 0.1 to 1.9
- expert_ids: int32 [4096, 2], P(('sp', 'tp')), may hold values from 0 to 7, all different within a row; in each aligned block of 128 rows (0 to 127, 128 to 255, ...) at most 64 rows name the same one
- route_weight: float32 [4096, 2], P(('sp', 'tp')), may hold values from 0.05 to 0.5
- w_gate: bfloat16 [8, 2048, 2048], P('sp', None, 'tp'), may hold values from -0.5 to 0.5
- w_up: bfloat16 [8, 2048, 2048], P('sp', None, 'tp'), may hold values from -0.5 to 0.5
- w_down: bfloat16 [8, 2048, 2048], P('sp', 'tp'), may hold values from -0.03125 to 0.03125
- out_gain: float32 [2048], replicated, may hold values from 0.1 to 1.9
Outputs:
- blended: bfloat16 [4096, 2048], P(('sp', 'tp'))
The draws below stay inside these ranges and needn't reach their ends.
Inputs may be any that keep to these rules, and one draw needn't show every extreme that they name: `expert_ids`: in each aligned block of 128 rows (the rows of one device) no expert is named by more than 64 rows, a bound that some block reaches.
All inputs are finite; a program needn't handle non-finite values.
Results may differ from the reference program's by a relative error of at most 0.015.
Values may be sent and summed in bfloat16 or wider, within the bound.
No kernel may reach another device: no remote copies, remote signals or barrier semaphores. Data moves between devices by JAX's collectives and lax.ppermute only.
A program may use at most 128 MiB of HBM per device.

```python
import math
from functools import partial
import jax
import jax.numpy as jnp
import numpy as np
from jax import lax

D = 2048
DC = 2048
FFE = 2048
KERNEL = 31
TOPK = 2
TOKENS = 4096
BLOCK = 128
EXPERTS = 8
CAP = 64
N_SP = 8
N_TP = 4


def draw_glu_value(key, part):
    key_rough, key_base = jax.random.split(key, 2)
    ramp = 10.0 ** (jnp.arange(DC, dtype=jnp.float32) / DC)
    rough = jax.random.uniform(key_rough, (DC,), jnp.float32, 0.5, 1.5)
    base = jnp.clip(jax.random.normal(key_base, (TOKENS, DC), jnp.float32), -6.0, 6.0)
    return (0.5 * ramp * rough * base).astype(jnp.bfloat16)


def shard_levels(own_key, extent, cuts, least, high):
    level = 1.0
    for dim, shards_of in cuts:
        steps = jax.random.uniform(jax.random.fold_in(jax.random.fold_in(own_key, 6), dim), (shards_of,), jnp.float32, least / len(cuts), high / len(cuts))
        level = level * jnp.repeat(jnp.exp(steps), extent[dim] // shards_of).reshape((-1,) + (1,) * (len(extent) - 1 - dim))
    return level


def routed_block(rng, own, number, rows, number_of, top, bound, skew):
    order = jax.random.permutation(rng, number_of)
    crowded, usual = portions_of(number_of, rows * top, bound, skew, True), portions_of(number_of, rows * top, bound, skew, False)
    places = jnp.arange(number_of)

    def named(tallies, turn):
        used = int((tallies > 0).sum())
        fixed = max(1, used // 4)
        moved = fixed + (places - fixed + turn * (used - fixed)) % max(1, number_of - fixed)
        return jnp.zeros((number_of,), jnp.int32).at[order[jnp.where(places < fixed, places, moved)]].set(jnp.asarray(tallies, jnp.int32))

    tallies = jnp.where(number % 4 == 0, named(crowded, number // 4), named(usual, number - number // 4 - 1))
    mixed = jax.random.permutation(jax.random.fold_in(own, 3), number_of)
    giver, sink = mixed[0:number_of // 2 * 2:2], mixed[1:number_of // 2 * 2:2]
    margin = jnp.minimum(tallies[giver] - 1, bound - tallies[sink]) // 2
    margin = jnp.where((giver == order[0]) | (sink == order[0]) | (tallies[sink] == 0), 0, jnp.maximum(margin, 0))
    moved = jax.random.randint(jax.random.fold_in(own, 4), (number_of // 2,), 0, 1 << 20) % (margin + 1)
    tallies = tallies.at[giver].add(-moved).at[sink].add(moved)
    items = jnp.searchsorted(jnp.cumsum(tallies), jnp.arange(rows * top), side="right").astype(jnp.int32)
    grid = items.reshape(top, rows).T
    grid = grid[jax.random.permutation(jax.random.fold_in(own, 1), rows)]
    turn = jax.random.randint(jax.random.fold_in(own, 2), (rows, 1), 0, top)
    return jnp.take_along_axis(grid, (jnp.arange(top)[None, :] + turn) % top, axis=1)


def portions_of(number_of, total, reach, skew, full):
    loads = [(1 << 20) // math.isqrt(rank ** skew) + 1 for rank in range(1, number_of + 1)]
    largest = reach if full else min(reach, max(-(-total // number_of), total * loads[0] // sum(loads)))
    least = 1 if total - largest >= number_of - 1 else 0
    holding, spare = [largest] + [least] * (number_of - 1), total - largest - least * (number_of - 1)
    while spare > 0:
        candidates = [i for i in range(1, number_of) if holding[i] < largest] or [i for i in range(1, number_of) if holding[i] < reach]
        mass, budget = sum([loads[i] for i in candidates]), spare
        for i in candidates:
            addition = min(reach - holding[i], max(1, budget * loads[i] // mass), spare)
            holding[i] = holding[i] + addition
            spare = spare - addition
    return np.array(holding)


def noise(stream_key, dims, scale, limit, cuts=(), kind=jnp.bfloat16):
    factor_of = shard_levels(stream_key, dims, cuts, -0.22, 0.18) if cuts else 1.0
    values = jax.random.normal(stream_key, dims, jnp.float32) * scale * factor_of
    return jnp.minimum(jnp.maximum(values, -limit), limit).astype(kind)


def setup_inputs(seed: int = 0) -> dict:
    splits = jax.random.split(jax.random.key(seed), 14)
    glu_value = draw_glu_value(jax.random.fold_in(splits[13], 71), 0)
    glu_gate = noise(splits[1], (TOKENS, DC), 1.5, 9.0, ((0, 8), (1, 4)))
    conv_kernel = noise(splits[2], (KERNEL, DC), KERNEL ** -0.5, 1.0, ((1, 4),), jnp.float32)
    norm_gain = jnp.clip(1.0 + 0.18 * jax.random.normal(splits[3], (DC,), jnp.float32), 0.1, 1.9)
    mix_weight = noise(splits[4], (DC, D), DC ** -0.5, 0.125, ((0, 4),))
    residual = noise(splits[5], (TOKENS, D), 1.0, 6.0, ((0, 32),))
    resid_gain = jnp.clip(1.0 + 0.18 * jax.random.normal(splits[6], (D,), jnp.float32), 0.1, 1.9)
    expert_ids_keys = jax.random.split(jax.random.fold_in(splits[7], 1), TOKENS // BLOCK)
    expert_ids_turns = jax.random.permutation(jax.random.fold_in(splits[7], 3), TOKENS // BLOCK)
    expert_ids = jax.vmap(lambda own, number: routed_block(jax.random.fold_in(splits[7], 2), own, number, BLOCK, EXPERTS, TOPK, CAP, 2))(expert_ids_keys, expert_ids_turns).reshape((TOKENS, TOPK))
    route_weight = jnp.clip(jnp.exp(math.log(0.5) - 2.3025851 * jax.random.uniform(splits[8], (TOKENS, TOPK), jnp.float32) ** shard_levels(splits[8], (TOKENS, TOPK), ((0, 32),), -0.2, 0.2)), 0.05, 0.5)
    w_gate = noise(splits[9], (EXPERTS, D, FFE), (D // 16) ** -0.5, 0.5, ((0, 8), (2, 4)))
    w_up = noise(splits[10], (EXPERTS, D, FFE), (D // 16) ** -0.5, 0.5, ((0, 8), (2, 4)))
    w_down = noise(splits[11], (EXPERTS, FFE, D), (16 * FFE) ** -0.5, 0.03125, ((0, 8), (1, 4)))
    out_gain = jnp.clip(1.0 + 0.18 * jax.random.normal(splits[12], (D,), jnp.float32), 0.1, 1.9)
    return {"glu_value": glu_value, "glu_gate": glu_gate, "conv_kernel": conv_kernel, "norm_gain": norm_gain, "mix_weight": mix_weight, "residual": residual, "resid_gain": resid_gain, "expert_ids": expert_ids, "route_weight": route_weight, "w_gate": w_gate, "w_up": w_up, "w_down": w_down, "out_gain": out_gain}


EPSILON = 1e-05
LIMIT = 7.0
SLOPE = 1.702

def normalize(values, gain_vector):
    centre = lax.optimization_barrier(jnp.mean(values, axis=-1, keepdims=True))
    spread = lax.optimization_barrier(jnp.mean(jnp.square(values - centre), axis=-1, keepdims=True))
    return (values - centre) * lax.rsqrt(spread + EPSILON) * gain_vector

def slot_layout(route_ids, experts, capacity):
    row_count, top_count = route_ids.shape
    flat_ids = route_ids.reshape(row_count * top_count).astype(jnp.int32)
    onehot = (flat_ids[:, None] == jnp.arange(experts, dtype=jnp.int32)[None, :]).astype(jnp.int32)
    before = jnp.cumsum(onehot, axis=0) - onehot
    slot_rank = lax.optimization_barrier(jnp.sum(before * onehot, axis=1)).astype(jnp.int32)
    position = (flat_ids * capacity + slot_rank).astype(jnp.int32)
    owners = (jnp.arange(row_count * top_count, dtype=jnp.int32) // top_count).astype(jnp.int32)
    slot_table = jnp.full((experts * capacity,), row_count, jnp.int32).at[position].set(owners)
    return (slot_table, position.reshape(row_count, top_count))

def run_expert(operands):
    tokens, gate_matrix, up_matrix, down_matrix = operands
    tokens_wide = tokens.astype(jnp.float32)
    gate_pre = jnp.dot(tokens_wide, gate_matrix.astype(jnp.float32), preferred_element_type=jnp.float32)
    up_pre = jnp.dot(tokens_wide, up_matrix.astype(jnp.float32), preferred_element_type=jnp.float32)
    gated = jnp.minimum(gate_pre, LIMIT)
    upper = jnp.clip(up_pre, -LIMIT, LIMIT)
    activity = ((upper + 1.0) * gated * jax.nn.sigmoid(SLOPE * gated)).astype(jnp.bfloat16)
    quarter = FFE // N_TP
    pieces = activity.reshape(-1, N_TP, quarter).astype(jnp.float32)
    downs = down_matrix.reshape(N_TP, quarter, D).astype(jnp.float32)
    partials = jnp.einsum('rqf,qfd->qrd', pieces, downs).astype(jnp.bfloat16)
    partials = lax.optimization_barrier(partials)
    return lax.optimization_barrier(jnp.sum(partials.astype(jnp.float32), axis=0)).astype(jnp.bfloat16)

def reference(glu_value, glu_gate, conv_kernel, norm_gain, mix_weight, residual, resid_gain, expert_ids, route_weight, w_gate, w_up, w_down, out_gain):
    gated_in = (glu_value.astype(jnp.float32) * jax.nn.sigmoid(glu_gate.astype(jnp.float32))).astype(jnp.bfloat16)
    extended = jnp.pad(gated_in.astype(jnp.float32), ((KERNEL - 1, 0), (0, 0)))
    convolved = jnp.zeros((TOKENS, DC), jnp.float32)
    for offset in range(KERNEL):
        convolved = convolved + conv_kernel[offset] * extended[offset:offset + TOKENS]
    centre = lax.optimization_barrier(jnp.mean(convolved, axis=1, keepdims=True))
    spread = lax.optimization_barrier(jnp.mean(jnp.square(convolved), axis=1, keepdims=True)) - centre * centre
    normed = (convolved - centre) * lax.rsqrt(spread + EPSILON) * norm_gain
    mix_in = jax.nn.silu(normed).astype(jnp.bfloat16)
    mixed_rows = jnp.dot(mix_in, mix_weight, preferred_element_type=jnp.float32)
    hidden = normalize(residual.astype(jnp.float32) + mixed_rows, resid_gain).astype(jnp.bfloat16)
    block_count = N_SP * N_TP
    block_ids = expert_ids.reshape(block_count, BLOCK, TOPK)
    tables, positions = jax.vmap(partial(slot_layout, experts=EXPERTS, capacity=CAP))(block_ids)
    hidden_blocks = hidden.reshape(block_count, BLOCK, D)
    padded = jnp.concatenate([hidden_blocks, jnp.zeros((block_count, 1, D), jnp.bfloat16)], axis=1)
    slot_rows = jax.vmap(partial(jnp.take, axis=0))(padded, tables)
    expert_major = slot_rows.reshape(block_count, EXPERTS, CAP, D).transpose(1, 0, 2, 3)
    expert_major = expert_major.reshape(EXPERTS, block_count * CAP, D)
    outputs = lax.map(run_expert, (expert_major, w_gate, w_up, w_down))
    block_major = outputs.reshape(EXPERTS, block_count, CAP, D).transpose(1, 0, 2, 3)
    block_major = block_major.reshape(block_count, EXPERTS * CAP, D)
    picked = jax.vmap(partial(jnp.take, axis=0))(block_major, positions.reshape(block_count, BLOCK * TOPK))
    picked = picked.reshape(TOKENS, TOPK, D)
    routed_sum = jnp.einsum('tk,tkd->td', route_weight.astype(jnp.float32), picked.astype(jnp.float32))
    return normalize(hidden.astype(jnp.float32) + routed_sum, out_gain).astype(jnp.bfloat16)
```

```python
import jax
import jax.numpy as jnp
from jax import lax
from jax.sharding import PartitionSpec as P

EPSILON = 1e-05
LIMIT = 7.0
SLOPE = 1.702


def shifted(block, axis, distance):
    devices = range(lax.axis_size(axis))
    route = [(i - distance, i) for i in devices if i - distance in devices]
    return lax.ppermute(block, axis, route)


def swapped(block, axis, bit):
    return lax.ppermute(block, axis, [(i, i ^ bit) for i in range(lax.axis_size(axis))])


def folded_ring(length):
    return list(range(0, length, 2)) + list(range(1, length, 2))[::-1]


def around(block, distance):
    count = lax.axis_size("sp")
    order = folded_ring(count // 2)
    route = []
    for place, line in enumerate(order):
        target = order[(place + distance) % len(order)]
        route += [(2 * line, 2 * target), (2 * line + 1, 2 * target + 1)]
    return lax.ppermute(block, "sp", route)


def normalize(values, gain_vector):
    centre = jnp.mean(values, axis=-1, keepdims=True)
    spread = jnp.mean(jnp.square(values - centre), axis=-1, keepdims=True)
    return (values - centre) * lax.rsqrt(spread + EPSILON) * gain_vector


def matmul(a, b):
    return jnp.dot(a, b, preferred_element_type=jnp.float32)


def expert_activity(tokens, gate_matrix, up_matrix):
    gated = jnp.minimum(matmul(tokens, gate_matrix), LIMIT)
    upper = jnp.clip(matmul(tokens, up_matrix), -LIMIT, LIMIT)
    return ((upper + 1.0) * gated * jax.nn.sigmoid(SLOPE * gated)).astype(jnp.bfloat16)


def convolve(glu_value, glu_gate, conv_kernel, norm_gain):
    gated_in = (
        glu_value.astype(jnp.float32) * jax.nn.sigmoid(glu_gate.astype(jnp.float32))
    ).astype(jnp.bfloat16)
    reach_back = conv_kernel.shape[0] - 1
    length, channels = gated_in.shape
    before_rows = shifted(gated_in[length - reach_back :], "sp", 1)
    extended = jnp.concatenate([before_rows, gated_in], axis=0).astype(jnp.float32)
    convolved = jnp.zeros(gated_in.shape, jnp.float32)
    for offset in range(reach_back + 1):
        convolved = convolved + conv_kernel[offset] * extended[offset : offset + length]
    channel_sum, squares = lax.psum(
        (jnp.sum(convolved, axis=1), jnp.sum(convolved * convolved, axis=1)), "tp"
    )
    channels = channels * lax.axis_size("tp")
    centre = channel_sum / channels
    spread = squares / channels - centre * centre
    normed = (convolved - centre[:, None]) * lax.rsqrt(spread[:, None] + EPSILON) * norm_gain
    return jax.nn.silu(normed).astype(jnp.bfloat16)


def scattered_product(mix_in, mix_weight):
    count = lax.axis_size("tp")
    rows = mix_in.shape[0] // count
    here = lax.axis_index("tp")

    def product(d):
        own = lax.dynamic_slice_in_dim(mix_in, (here ^ d) * rows, rows, axis=0)
        return matmul(own, mix_weight)

    parts = [None] * count
    for d in reversed(range(count)):
        parts[d] = product(d)
    bit = 1
    while bit < count:
        kept = {}
        for d in reversed(range(0, count, 2 * bit)):
            arrived = swapped(parts[d + bit].astype(jnp.bfloat16), "tp", bit)
            kept[d] = parts[d] + arrived.astype(jnp.float32)
        parts = [kept.get(d) for d in range(count)]
        bit *= 2
    return parts[0]


def slots_of(ids, weights, expert, capacity):
    named = (ids == expert).astype(jnp.float32)
    chosen = jnp.sum(named, axis=1)
    count = ids.shape[0]
    earlier = (
        lax.broadcasted_iota(jnp.int32, (count, count), 0)
        > lax.broadcasted_iota(jnp.int32, (count, count), 1)
    ).astype(jnp.float32)
    rank = jnp.sum(earlier * chosen[None, :], axis=1)
    places = lax.broadcasted_iota(jnp.int32, (count, capacity), 1).astype(jnp.float32)
    onehot = ((places == rank[:, None]) & (chosen[:, None] > 0)).astype(jnp.bfloat16)
    return onehot, jnp.sum(named * weights, axis=1)


def routed_ring(hidden, ids, weights, gate_local, up_local, down_local, capacity):
    tp_count = lax.axis_size("tp")
    steps = lax.axis_size("sp") // 2
    here = lax.axis_index("sp").astype(jnp.float32)
    other = (lax.axis_index("sp") ^ 1).astype(jnp.float32)
    top = ids.shape[1]
    table = jnp.concatenate([ids.astype(jnp.float32), weights], axis=1)
    tables = [table] + [around(table, s) for s in range(1, steps)]
    slots = []
    for s in range(steps):
        pair = [slots_of(tables[s][:, :top], tables[s][:, top:], e, capacity) for e in (here, other)]
        slots.append(pair)
    block = hidden
    shares = []
    carried = None
    for s in range(steps):
        following = around(block, 1) if s + 1 < steps else None
        (own_hot, own_weight), (far_hot, far_weight) = slots[s]
        picked = [matmul(hot.T, block).astype(jnp.bfloat16) for hot in (own_hot, far_hot)]
        rows = jnp.concatenate([picked[0], swapped(picked[1], "sp", 1)], axis=0)
        bit = tp_count // 2
        while bit:
            rows = jnp.concatenate([rows, swapped(rows, "tp", bit)], axis=0)
            bit //= 2
        sums = matmul(expert_activity(rows, gate_local, up_local), down_local)
        bit = 1
        while bit < tp_count:
            half = sums.shape[0] // 2
            arrived = swapped(sums[half:].astype(jnp.bfloat16), "tp", bit)
            sums = sums[:half] + arrived.astype(jnp.float32)
            bit *= 2
        mine = sums[:capacity].astype(jnp.bfloat16)
        theirs = swapped(sums[capacity:].astype(jnp.bfloat16), "sp", 1)
        share = own_weight[:, None] * matmul(own_hot, mine) + far_weight[:, None] * matmul(far_hot, theirs)
        if s == 0:
            own_share = share
        elif carried is None:
            carried = share
        else:
            carried = carried + share
        if s:
            carried = around(carried.astype(jnp.bfloat16), 1).astype(jnp.float32)
        block = following
    return own_share + carried


def slot_layout(route_ids, experts, capacity):
    row_count, top_count = route_ids.shape
    flat_ids = route_ids.reshape(row_count * top_count)
    onehot = (flat_ids[:, None] == jnp.arange(experts, dtype=jnp.int32)[None, :]).astype(jnp.int32)
    before = jnp.cumsum(onehot, axis=0) - onehot
    slot_rank = jnp.sum(before * onehot, axis=1)
    position = flat_ids * capacity + slot_rank
    owners = jnp.arange(row_count * top_count, dtype=jnp.int32) // top_count
    slot_table = jnp.full((experts * capacity,), row_count, jnp.int32).at[position].set(owners)
    return (slot_table, position.reshape(row_count, top_count))


def routed_exchange(hidden, ids, weights, gate_local, up_local, down_local, capacity):
    experts = lax.axis_size("sp")
    own_count, width = hidden.shape
    top_count = ids.shape[1]
    own_table, positions = slot_layout(ids, experts, capacity)
    padded = jnp.concatenate([hidden, jnp.zeros((1, width), jnp.bfloat16)], axis=0)
    dispatched = padded[own_table].reshape(experts, capacity, width)
    arrived = lax.all_to_all(dispatched, "sp", split_axis=0, concat_axis=0, tiled=True)
    gathered = lax.all_gather(arrived[None], "tp", axis=0, tiled=True)
    activity = expert_activity(gathered.reshape(-1, width), gate_local, up_local)
    expert_out = lax.psum_scatter(
        matmul(activity, down_local).astype(jnp.bfloat16), "tp", scatter_dimension=0, tiled=True
    )
    expert_out = expert_out.reshape(experts, capacity, width)
    returned = lax.all_to_all(expert_out, "sp", split_axis=0, concat_axis=0, tiled=True)
    picked = returned.reshape(experts * capacity, width)[positions.reshape(-1)]
    picked = picked.reshape(own_count, top_count, width)
    return jnp.einsum("tk,tkd->td", weights, picked.astype(jnp.float32))


def shards(
    glu_value,
    glu_gate,
    conv_kernel,
    norm_gain,
    mix_weight,
    residual,
    resid_gain,
    expert_ids,
    route_weight,
    w_gate,
    w_up,
    w_down,
    out_gain,
):
    mix_in = convolve(glu_value, glu_gate, conv_kernel, norm_gain)
    mixed_rows = scattered_product(mix_in, mix_weight)
    hidden = normalize(residual.astype(jnp.float32) + mixed_rows, resid_gain).astype(jnp.bfloat16)
    experts = lax.axis_size("sp")
    own_count, top_count = expert_ids.shape
    capacity = 2 * own_count * top_count // experts
    whole_rows = (experts // 2 - 1) * own_count + experts // 2 * capacity
    padded_rows = (experts - 1) * capacity
    route = routed_ring if whole_rows <= 2 * padded_rows else routed_exchange
    routed_sum = route(hidden, expert_ids, route_weight, w_gate[0], w_up[0], w_down[0], capacity)
    return normalize(hidden.astype(jnp.float32) + routed_sum, out_gain).astype(jnp.bfloat16)


def solution(mesh):
    in_specs = (
        P("sp", "tp"),
        P("sp", "tp"),
        P(None, "tp"),
        P("tp"),
        P("tp", None),
        P(("sp", "tp"), None),
        P(),
        P(("sp", "tp"), None),
        P(("sp", "tp"), None),
        P("sp", None, "tp"),
        P("sp", None, "tp"),
        P("sp", "tp", None),
        P(),
    )
    out_specs = P(("sp", "tp"), None)
    return jax.shard_map(shards, mesh=mesh, in_specs=in_specs, out_specs=out_specs, check_vma=False)
```

```python
import jax
import jax.numpy as jnp
from jax import lax
from jax.experimental import pallas as pl
from jax.experimental.pallas import tpu as pltpu
from jax.sharding import PartitionSpec as P


EPSILON = 1e-05
LIMIT = 7.0
SLOPE = 1.702


def shifted(block, axis, distance):
    devices = range(lax.axis_size(axis))
    route = [(i - distance, i) for i in devices if i - distance in devices]
    return lax.ppermute(block, axis, route)


def swapped(block, axis, bit):
    return lax.ppermute(block, axis, [(i, i ^ bit) for i in range(lax.axis_size(axis))])


def folded_ring(length):
    return list(range(0, length, 2)) + list(range(1, length, 2))[::-1]


def around(block, distance):
    count = lax.axis_size("sp")
    order = folded_ring(count // 2)
    route = []
    for place, line in enumerate(order):
        target = order[(place + distance) % len(order)]
        route += [(2 * line, 2 * target), (2 * line + 1, 2 * target + 1)]
    return lax.ppermute(block, "sp", route)


def normalize(values, gain_vector):
    centre = jnp.mean(values, axis=-1, keepdims=True)
    spread = jnp.mean(jnp.square(values - centre), axis=-1, keepdims=True)
    return (values - centre) * lax.rsqrt(spread + EPSILON) * gain_vector


def matmul(a, b):
    return jnp.dot(a, b, preferred_element_type=jnp.float32)


def expert_activity(tokens, gate_matrix, up_matrix):
    gated = jnp.minimum(matmul(tokens, gate_matrix), LIMIT)
    upper = jnp.clip(matmul(tokens, up_matrix), -LIMIT, LIMIT)
    return ((upper + 1.0) * gated * jax.nn.sigmoid(SLOPE * gated)).astype(jnp.bfloat16)


def expert_kernel(near, far, gate_matrix, up_matrix, down_matrix, keep, pass_on, send):
    def product(tokens):
        gated = jnp.minimum(matmul(tokens, gate_matrix[...]), LIMIT)
        upper = jnp.clip(matmul(tokens, up_matrix[...]), -LIMIT, LIMIT)
        activity = (upper + 1.0) * gated / (1.0 + jnp.exp(-SLOPE * gated))
        return matmul(activity.astype(jnp.bfloat16), down_matrix[...])

    send[...] = product(far[...]).astype(jnp.bfloat16)
    sums = product(near[...])
    half = keep.shape[0]
    keep[...] = sums[:half]
    pass_on[...] = sums[half:]


def expert_step(near, far, gate_matrix, up_matrix, down_matrix):
    rows, width = near.shape
    vmem = pl.BlockSpec(memory_space=pltpu.VMEM)
    return pl.pallas_call(
        expert_kernel,
        out_shape=(
            jax.ShapeDtypeStruct((rows // 2, width), jnp.float32),
            jax.ShapeDtypeStruct((rows // 2, width), jnp.float32),
            jax.ShapeDtypeStruct((rows, width), jnp.bfloat16),
        ),
        in_specs=[vmem] * 5,
        out_specs=(vmem,) * 3,
        compiler_params=pltpu.CompilerParams(vmem_limit_bytes=40 * 2**20),
        cost_estimate=pl.CostEstimate(
            flops=12 * rows * width * gate_matrix.shape[1], transcendentals=0, bytes_accessed=0
        ),
        name="expert_step",
    )(near, far, gate_matrix, up_matrix, down_matrix)


def gated_rows(value, gate):
    return (value.astype(jnp.float32) * jax.nn.sigmoid(gate.astype(jnp.float32))).astype(jnp.bfloat16)


def convolve(glu_value, glu_gate, conv_kernel, norm_gain):
    reach_back = conv_kernel.shape[0] - 1
    length, channels = glu_value.shape
    tail = slice(length - reach_back, length)
    before_rows = shifted(gated_rows(glu_value[tail], glu_gate[tail]), "sp", 1)
    gated_in = gated_rows(glu_value, glu_gate)
    extended = jnp.concatenate([before_rows, gated_in], axis=0).astype(jnp.float32)
    convolved = jnp.zeros(gated_in.shape, jnp.float32)
    for offset in range(reach_back + 1):
        convolved = convolved + conv_kernel[offset] * extended[offset : offset + length]
    channel_sum, squares = lax.psum(
        (jnp.sum(convolved, axis=1), jnp.sum(convolved * convolved, axis=1)), "tp"
    )
    channels = channels * lax.axis_size("tp")
    centre = channel_sum / channels
    spread = squares / channels - centre * centre
    normed = (convolved - centre[:, None]) * lax.rsqrt(spread[:, None] + EPSILON) * norm_gain
    return jax.nn.silu(normed).astype(jnp.bfloat16)


def scattered_product(mix_in, mix_weight):
    count = lax.axis_size("tp")
    rows = mix_in.shape[0] // count
    here = lax.axis_index("tp")

    def product(d):
        own = lax.dynamic_slice_in_dim(mix_in, (here ^ d) * rows, rows, axis=0)
        return matmul(own, mix_weight)

    parts = [None] * count
    for d in reversed(range(count)):
        parts[d] = product(d)
    bit = 1
    while bit < count:
        kept = {}
        for d in reversed(range(0, count, 2 * bit)):
            arrived = swapped(parts[d + bit].astype(jnp.bfloat16), "tp", bit)
            kept[d] = parts[d] + arrived.astype(jnp.float32)
        parts = [kept.get(d) for d in range(count)]
        bit *= 2
    return parts[0]


def slots_of(ids, weights, expert, capacity):
    named = (ids == expert).astype(jnp.float32)
    chosen = jnp.sum(named, axis=1)
    count = ids.shape[0]
    earlier = (
        lax.broadcasted_iota(jnp.int32, (count, count), 0)
        > lax.broadcasted_iota(jnp.int32, (count, count), 1)
    ).astype(jnp.float32)
    rank = jnp.sum(earlier * chosen[None, :], axis=1)
    places = lax.broadcasted_iota(jnp.int32, (count, capacity), 1).astype(jnp.float32)
    onehot = ((places == rank[:, None]) & (chosen[:, None] > 0)).astype(jnp.bfloat16)
    return onehot, jnp.sum(named * weights, axis=1)


def routed_ring(hidden, ids, weights, gate_local, up_local, down_local, capacity):
    steps = lax.axis_size("sp") // 2
    here = lax.axis_index("sp").astype(jnp.float32)
    other = (lax.axis_index("sp") ^ 1).astype(jnp.float32)
    top = ids.shape[1]
    table = jnp.concatenate([ids.astype(jnp.float32), weights], axis=1)
    tables = [table]
    for s in range(1, steps):
        tables.append(around(table, s))
    block = hidden
    carried = None
    for s in range(steps):
        if s + 1 < steps:
            following = around(block, 1)
        own_hot, own_weight = slots_of(tables[s][:, :top], tables[s][:, top:], here, capacity)
        far_hot, far_weight = slots_of(tables[s][:, :top], tables[s][:, top:], other, capacity)
        far_rows = matmul(far_hot.T, block).astype(jnp.bfloat16)
        arrived = swapped(far_rows, "sp", 1)
        picked = matmul(own_hot.T, block).astype(jnp.bfloat16)
        own_x = swapped(picked, "tp", 2)
        far_x = swapped(arrived, "tp", 2)
        near = jnp.concatenate([picked, arrived, own_x, far_x], axis=0)
        far = swapped(near, "tp", 1)
        keep, pass_on, send = expert_step(near, far, gate_local, up_local, down_local)
        from_core = swapped(send, "tp", 1)
        half = keep.shape[0]
        pass_on = (pass_on + from_core[half:].astype(jnp.float32)).astype(jnp.bfloat16)
        from_chip = swapped(pass_on, "tp", 2)
        sums = keep + from_core[:half].astype(jnp.float32) + from_chip.astype(jnp.float32)
        sums = sums.astype(jnp.bfloat16)
        mine, theirs = sums[:capacity], sums[capacity:]
        theirs = swapped(theirs, "sp", 1)
        share = own_weight[:, None] * matmul(own_hot, mine) + far_weight[:, None] * matmul(far_hot, theirs)
        if s == 0:
            own_share = share
        else:
            share = (share if carried is None else carried.astype(jnp.float32) + share).astype(jnp.bfloat16)
        if s:
            carried = around(share, 1)
        block = following
    return own_share + carried.astype(jnp.float32)


def slot_layout(route_ids, experts, capacity):
    row_count, top_count = route_ids.shape
    flat_ids = route_ids.reshape(row_count * top_count)
    onehot = (flat_ids[:, None] == jnp.arange(experts, dtype=jnp.int32)[None, :]).astype(jnp.int32)
    before = jnp.cumsum(onehot, axis=0) - onehot
    slot_rank = jnp.sum(before * onehot, axis=1)
    position = flat_ids * capacity + slot_rank
    owners = jnp.arange(row_count * top_count, dtype=jnp.int32) // top_count
    slot_table = jnp.full((experts * capacity,), row_count, jnp.int32).at[position].set(owners)
    return (slot_table, position.reshape(row_count, top_count))


def routed_exchange(hidden, ids, weights, gate_local, up_local, down_local, capacity):
    experts = lax.axis_size("sp")
    own_count, width = hidden.shape
    top_count = ids.shape[1]
    own_table, positions = slot_layout(ids, experts, capacity)
    padded = jnp.concatenate([hidden, jnp.zeros((1, width), jnp.bfloat16)], axis=0)
    dispatched = padded[own_table].reshape(experts, capacity, width)
    arrived = lax.all_to_all(dispatched, "sp", split_axis=0, concat_axis=0, tiled=True)
    gathered = lax.all_gather(arrived[None], "tp", axis=0, tiled=True)
    activity = expert_activity(gathered.reshape(-1, width), gate_local, up_local)
    expert_out = lax.psum_scatter(
        matmul(activity, down_local).astype(jnp.bfloat16), "tp", scatter_dimension=0, tiled=True
    )
    expert_out = expert_out.reshape(experts, capacity, width)
    returned = lax.all_to_all(expert_out, "sp", split_axis=0, concat_axis=0, tiled=True)
    picked = returned.reshape(experts * capacity, width)[positions.reshape(-1)]
    picked = picked.reshape(own_count, top_count, width)
    return jnp.einsum("tk,tkd->td", weights, picked.astype(jnp.float32))


def shards(
    glu_value,
    glu_gate,
    conv_kernel,
    norm_gain,
    mix_weight,
    residual,
    resid_gain,
    expert_ids,
    route_weight,
    w_gate,
    w_up,
    w_down,
    out_gain,
):
    mix_in = convolve(glu_value, glu_gate, conv_kernel, norm_gain)
    mix_in, expert_ids, route_weight = lax.optimization_barrier((mix_in, expert_ids, route_weight))
    mixed_rows = scattered_product(mix_in, mix_weight)
    hidden = normalize(residual.astype(jnp.float32) + mixed_rows, resid_gain).astype(jnp.bfloat16)
    experts = lax.axis_size("sp")
    own_count, top_count = expert_ids.shape
    capacity = 2 * own_count * top_count // experts
    whole_rows = (experts // 2 - 1) * own_count + experts // 2 * capacity
    padded_rows = (experts - 1) * capacity
    ring = lax.axis_size("tp") == 4 and whole_rows <= 2 * padded_rows
    route = routed_ring if ring else routed_exchange
    routed_sum = route(hidden, expert_ids, route_weight, w_gate[0], w_up[0], w_down[0], capacity)
    return normalize(hidden.astype(jnp.float32) + routed_sum, out_gain).astype(jnp.bfloat16)


def solution(mesh):
    in_specs = (
        P("sp", "tp"),
        P("sp", "tp"),
        P(None, "tp"),
        P("tp"),
        P("tp", None),
        P(("sp", "tp"), None),
        P(),
        P(("sp", "tp"), None),
        P(("sp", "tp"), None),
        P("sp", None, "tp"),
        P("sp", None, "tp"),
        P("sp", "tp", None),
        P(),
    )
    out_specs = P(("sp", "tp"), None)
    return jax.shard_map(shards, mesh=mesh, in_specs=in_specs, out_specs=out_specs, check_vma=False)
```

```python
import jax
import jax.numpy as jnp
from jax import lax
from jax.experimental import pallas as pl
from jax.experimental.pallas import tpu as pltpu
from jax.sharding import PartitionSpec as P


EPSILON = 1e-05
LIMIT = 7.0
SLOPE = 1.702


def shifted(block, axis, distance):
    devices = range(lax.axis_size(axis))
    route = [(i - distance, i) for i in devices if i - distance in devices]
    return lax.ppermute(block, axis, route)


def swapped(block, axis, bit):
    return lax.ppermute(block, axis, [(i, i ^ bit) for i in range(lax.axis_size(axis))])


def folded_ring(length):
    return list(range(0, length, 2)) + list(range(1, length, 2))[::-1]


def around(block, distance):
    count = lax.axis_size("sp")
    order = folded_ring(count // 2)
    route = []
    for place, line in enumerate(order):
        target = order[(place + distance) % len(order)]
        route += [(2 * line, 2 * target), (2 * line + 1, 2 * target + 1)]
    return lax.ppermute(block, "sp", route)


def normalize(values, gain_vector):
    centre = jnp.mean(values, axis=-1, keepdims=True)
    spread = jnp.mean(jnp.square(values - centre), axis=-1, keepdims=True)
    return (values - centre) * lax.rsqrt(spread + EPSILON) * gain_vector


def matmul(a, b):
    return jnp.dot(a, b, preferred_element_type=jnp.float32)


def expert_activity(tokens, gate_matrix, up_matrix):
    gated = jnp.minimum(matmul(tokens, gate_matrix), LIMIT)
    upper = jnp.clip(matmul(tokens, up_matrix), -LIMIT, LIMIT)
    return ((upper + 1.0) * gated * jax.nn.sigmoid(SLOPE * gated)).astype(jnp.bfloat16)


def expert_kernel(tokens, gate_matrix, up_matrix, down_matrix, *outs):
    gated = jnp.minimum(matmul(tokens[...], gate_matrix[...]), LIMIT)
    upper = jnp.clip(matmul(tokens[...], up_matrix[...]), -LIMIT, LIMIT)
    activity = (upper + 1.0) * gated / (1.0 + jnp.exp(-SLOPE * gated))
    sums = matmul(activity.astype(jnp.bfloat16), down_matrix[...])
    rows = sums.shape[0] // len(outs)
    for i, out in enumerate(outs):
        out[...] = sums[i * rows : (i + 1) * rows].astype(out.dtype)


def expert_step(tokens, gate_matrix, up_matrix, down_matrix, dtype, parts):
    rows, width = tokens.shape
    vmem = pl.BlockSpec(memory_space=pltpu.VMEM)
    return pl.pallas_call(
        expert_kernel,
        out_shape=(jax.ShapeDtypeStruct((rows // parts, width), dtype),) * parts,
        in_specs=[vmem] * 4,
        out_specs=(vmem,) * parts,
        compiler_params=pltpu.CompilerParams(vmem_limit_bytes=16 * 2**20),
        cost_estimate=pl.CostEstimate(
            flops=6 * rows * width * gate_matrix.shape[1], transcendentals=0, bytes_accessed=0
        ),
        name="expert_step",
    )(tokens, gate_matrix, up_matrix, down_matrix)


def gated_rows(value, gate):
    return (value.astype(jnp.float32) * jax.nn.sigmoid(gate.astype(jnp.float32))).astype(jnp.bfloat16)


def convolve_rows(extended, taps, first, row, rows, window):
    lanes = window.stop - window.start
    sums = jnp.zeros((rows, lanes), jnp.float32)
    for shift in range(8):
        part = jnp.zeros(((rows + 8) // 8, 8, lanes), jnp.float32)
        for k in range(taps.shape[0]):
            if (first + k) % 8 == shift:
                block = extended[pl.ds(row + first + k - shift, rows + 8), window]
                tap = jnp.broadcast_to(taps[k : k + 1, window], (8, lanes))
                part = part + block.reshape(part.shape) * tap[None]
        sums = sums + part.reshape(rows + 8, lanes)[shift : shift + rows]
    return sums


def convolve_kernel(gated, kernel, gain, weight, out, total, squares, taps, gains, weights, extended, arrived, *, pad, rows):
    length, channels = gated.shape
    moves = [
        pltpu.make_async_copy(source, target, arrived.at[i])
        for i, (source, target) in enumerate(((kernel, taps), (gain, gains), (weight, weights)))
    ]
    for move in moves:
        move.start()
    extended[pl.ds(0, pad), :] = jnp.zeros((pad, channels), jnp.float32)
    extended[pl.ds(pad, length), :] = gated[...].astype(jnp.float32)
    moves[0].wait()
    first = pad - (taps.shape[0] - 1)

    def body(i, carry):
        row = pl.multiple_of(i * rows, rows)
        own_total = jnp.zeros((rows, 128), jnp.float32)
        own_squares = jnp.zeros((rows, 128), jnp.float32)
        for lane in range(0, channels, 128):
            window = slice(lane, lane + 128)
            sums = convolve_rows(extended, taps, first, row, rows, window)
            out[pl.ds(row, rows), window] = sums
            own_total = own_total + sums
            own_squares = own_squares + sums * sums
        total[pl.ds(row, rows), :] = own_total
        squares[pl.ds(row, rows), :] = own_squares
        return carry

    lax.fori_loop(0, length // rows, body, 0)
    moves[1].wait()
    moves[2].wait()


def head_kernel(before, gated, taps, total, squares, head, stats, extended):
    pad, channels = before.shape
    first = pad - (taps.shape[0] - 1)
    extended[0:pad, :] = before[...].astype(jnp.float32)
    extended[pad : 2 * pad, :] = gated[0:pad, :].astype(jnp.float32)
    total[0:pad, :] = jnp.zeros((pad, 128), jnp.float32)
    squares[0:pad, :] = jnp.zeros((pad, 128), jnp.float32)
    for lane in range(0, channels, 128):
        window = slice(lane, lane + 128)
        sums = convolve_rows(extended, taps, first, 0, pad, window)
        head[:, window] = sums
        total[0:pad, :] += sums
        squares[0:pad, :] += sums * sums
    ones = jnp.ones((8, 128), jnp.float32)
    for place, partial in enumerate((total, squares)):
        sums = lax.dot_general(
            ones,
            partial[...],
            (((1,), (1,)), ((), ())),
            precision=lax.Precision.HIGHEST,
            preferred_element_type=jnp.float32,
        )
        stats[place : place + 1, :] = sums[:1]


def in_vmem(*arrays):
    return tuple(pltpu.with_memory_space_constraint(a, pltpu.VMEM) for a in arrays)


def convolve(glu_value, glu_gate, conv_kernel, norm_gain, mix_weight):
    length, channels = glu_value.shape
    rows = min(128, length)
    pad = -(-(conv_kernel.shape[0] - 1) // 16) * 16
    tail = slice(length - pad, length)
    before_rows = shifted(gated_rows(glu_value[tail], glu_gate[tail]), "sp", 1)
    gated = gated_rows(glu_value, glu_gate)
    norm_gain = norm_gain[None]
    vmem, hbm = pl.BlockSpec(memory_space=pltpu.VMEM), pl.BlockSpec(memory_space=pltpu.HBM)
    convolved, total, squares, taps, gains, weights = pl.pallas_call(
        lambda *refs: convolve_kernel(*refs, pad=pad, rows=rows),
        out_shape=(
            jax.ShapeDtypeStruct((length, channels), jnp.float32),
            pltpu.VMEM((length, 128), jnp.float32),
            pltpu.VMEM((length, 128), jnp.float32),
            pltpu.VMEM(conv_kernel.shape, jnp.float32),
            pltpu.VMEM(norm_gain.shape, jnp.float32),
            pltpu.VMEM(mix_weight.shape, mix_weight.dtype),
        ),
        in_specs=[vmem, hbm, hbm, hbm],
        out_specs=(vmem,) * 6,
        scratch_shapes=[
            pltpu.VMEM((length + pad + 8, channels), jnp.float32),
            pltpu.SemaphoreType.DMA((3,)),
        ],
        compiler_params=pltpu.CompilerParams(vmem_limit_bytes=16 * 2**20),
        name="convolve",
    )(*in_vmem(gated), *(pltpu.with_memory_space_constraint(a, pltpu.HBM) for a in (conv_kernel, norm_gain, mix_weight)))
    head, own = pl.pallas_call(
        head_kernel,
        out_shape=(pltpu.VMEM((pad, channels), jnp.float32), pltpu.VMEM((2, length), jnp.float32)),
        in_specs=[vmem] * 5,
        out_specs=(vmem,) * 2,
        scratch_shapes=[pltpu.VMEM((2 * pad + 8, channels), jnp.float32)],
        compiler_params=pltpu.CompilerParams(vmem_limit_bytes=8 * 2**20),
        name="head",
    )(*in_vmem(before_rows, gated, taps, total, squares))
    stats = [own] + [swapped(own, "tp", d) for d in range(1, lax.axis_size("tp"))]
    return convolved, head, stats, gains, weights


def first_products_kernel(here, convolved, head, gain, mix_weight, *refs, bit, far, shares):
    stats, (mix_in, send, keep, wide) = refs[:shares], refs[shares:]
    rows, channels = send.shape[0], convolved.shape[1] * shares
    sums = stats[0][...]
    for share in stats[1:]:
        sums = sums + share[...]
    centre = sums[0:1] / channels
    spread = sums[1:2] / channels - centre * centre
    wide[...] = jnp.zeros_like(wide)
    wide[0:1, :] = centre
    wide[1:2, :] = lax.rsqrt(spread + EPSILON)
    place = lax.broadcasted_iota(jnp.int32, (wide.shape[0], 128), 0)
    centre, scale = (
        lax.dot_general(
            wide[...],
            (place == i).astype(jnp.float32),
            (((0,), (0,)), ((), ())),
            precision=lax.Precision.HIGHEST,
            preferred_element_type=jnp.float32,
        )
        for i in (0, 1)
    )
    for lane in range(0, convolved.shape[1], 128):
        window = slice(lane, lane + 128)
        values = jnp.concatenate([head[:, window], convolved[head.shape[0] :, window]], axis=0)
        normed = (values - centre) * scale * gain[:, window]
        mix_in[:, window] = (normed / (1.0 + jnp.exp(-normed))).astype(jnp.bfloat16)
    for d, out in ((far + bit, send), (far, keep)):
        own = mix_in[pl.ds(pl.multiple_of((here[0] ^ d) * rows, rows), rows), :]
        out[...] = matmul(own, mix_weight[...]).astype(out.dtype)


def last_products_kernel(here, mix_in, mix_weight, send, keep, *, bit):
    rows = send.shape[0]
    for d, out in ((bit, send), (0, keep)):
        own = mix_in[pl.ds(pl.multiple_of((here[0] ^ d) * rows, rows), rows), :]
        out[...] = matmul(own, mix_weight[...]).astype(out.dtype)


def scattered_product(convolved, head, stats, norm_gain, mix_weight):
    count = lax.axis_size("tp")
    assert count == 4
    rows, width = convolved.shape[0] // count, mix_weight.shape[1]
    here = lax.axis_index("tp").reshape(1).astype(jnp.int32)
    vmem, smem = pl.BlockSpec(memory_space=pltpu.VMEM), pl.BlockSpec(memory_space=pltpu.SMEM)
    products = (pltpu.VMEM((rows, width), jnp.bfloat16), pltpu.VMEM((rows, width), jnp.float32))
    params = pltpu.CompilerParams(vmem_limit_bytes=8 * 2**20)
    mix_in, far_send, far_keep = pl.pallas_call(
        lambda *refs: first_products_kernel(*refs, bit=1, far=2, shares=count),
        out_shape=(pltpu.VMEM(convolved.shape, jnp.bfloat16),) + products,
        in_specs=[smem] + [vmem] * (4 + count),
        out_specs=(vmem,) * 3,
        scratch_shapes=[pltpu.VMEM((8, convolved.shape[0]), jnp.float32)],
        compiler_params=params,
        name="first_products",
    )(here, convolved, *in_vmem(head, norm_gain, mix_weight, *stats))
    arrived = swapped(far_send, "tp", 1)
    far_sum = (far_keep + arrived.astype(jnp.float32)).astype(jnp.bfloat16)
    from_chip = swapped(far_sum, "tp", 2)
    near_send, near_keep = pl.pallas_call(
        lambda *refs: last_products_kernel(*refs, bit=1),
        out_shape=products,
        in_specs=[smem, vmem, vmem],
        out_specs=(vmem,) * 2,
        compiler_params=params,
        name="last_products",
    )(here, *in_vmem(mix_in, mix_weight))
    arrived = swapped(near_send, "tp", 1)
    return near_keep, arrived, from_chip


def hidden_kernel(residual, keep, from_core, from_chip, gain, out):
    values = residual[...].astype(jnp.float32) + keep[...]
    values = values + from_core[...].astype(jnp.float32) + from_chip[...].astype(jnp.float32)
    out[...] = normalize(values, gain[...]).astype(out.dtype)


def slots_of(ids, weights, expert, capacity):
    named = (ids == expert).astype(jnp.float32)
    chosen = jnp.sum(named, axis=1)
    count = ids.shape[0]
    earlier = (
        lax.broadcasted_iota(jnp.int32, (count, count), 0)
        > lax.broadcasted_iota(jnp.int32, (count, count), 1)
    ).astype(jnp.float32)
    rank = jnp.sum(earlier * chosen[None, :], axis=1)
    places = lax.broadcasted_iota(jnp.int32, (count, capacity), 1).astype(jnp.float32)
    onehot = ((places == rank[:, None]) & (chosen[:, None] > 0)).astype(jnp.bfloat16)
    return onehot, jnp.sum(named * weights, axis=1)


def routed_ring(hidden, ids, weights, gate_local, up_local, down_local, capacity):
    steps = lax.axis_size("sp") // 2
    here = lax.axis_index("sp").astype(jnp.float32)
    other = (lax.axis_index("sp") ^ 1).astype(jnp.float32)
    top = ids.shape[1]
    table = jnp.concatenate([ids.astype(jnp.float32), weights], axis=1)
    tables = [table]
    for s in range(1, steps):
        tables.append(around(table, s))
    block = hidden
    carried = None
    for s in range(steps):
        if s + 1 < steps:
            following = around(block, 1)
        own_hot, own_weight = slots_of(tables[s][:, :top], tables[s][:, top:], here, capacity)
        far_hot, far_weight = slots_of(tables[s][:, :top], tables[s][:, top:], other, capacity)
        far_rows = matmul(far_hot.T, block).astype(jnp.bfloat16)
        arrived = swapped(far_rows, "sp", 1)
        picked = matmul(own_hot.T, block).astype(jnp.bfloat16)
        own_x = swapped(picked, "tp", 2)
        far_x = swapped(arrived, "tp", 2)
        near = jnp.concatenate([arrived, far_x, picked, own_x], axis=0)
        far = swapped(near, "tp", 1)
        near_sums = expert_step(near, gate_local, up_local, down_local, jnp.float32, 4)
        far_sums = expert_step(far, gate_local, up_local, down_local, jnp.bfloat16, 2)

        def crossed(send, leave):
            from_core = swapped(send, "tp", 1)
            leave = leave + from_core[capacity:].astype(jnp.float32)
            return from_core[:capacity], swapped(leave.astype(jnp.bfloat16), "tp", 2)

        def summed(keep, from_core, from_chip):
            total = keep + from_core.astype(jnp.float32) + from_chip.astype(jnp.float32)
            return total.astype(jnp.bfloat16)

        theirs = crossed(far_sums[0], near_sums[1])
        mine = crossed(far_sums[1], near_sums[3])
        far_sum = swapped(summed(near_sums[0], *theirs), "sp", 1)
        own_sum = summed(near_sums[2], *mine)
        share = own_weight[:, None] * matmul(own_hot, own_sum) + far_weight[:, None] * matmul(far_hot, far_sum)
        if s == 0:
            own_share = share
        else:
            share = (share if carried is None else carried.astype(jnp.float32) + share).astype(jnp.bfloat16)
        if s:
            carried = around(share, 1)
        block = following
    return own_share + carried.astype(jnp.float32)


def slot_layout(route_ids, experts, capacity):
    row_count, top_count = route_ids.shape
    flat_ids = route_ids.reshape(row_count * top_count)
    onehot = (flat_ids[:, None] == jnp.arange(experts, dtype=jnp.int32)[None, :]).astype(jnp.int32)
    before = jnp.cumsum(onehot, axis=0) - onehot
    slot_rank = jnp.sum(before * onehot, axis=1)
    position = flat_ids * capacity + slot_rank
    owners = jnp.arange(row_count * top_count, dtype=jnp.int32) // top_count
    slot_table = jnp.full((experts * capacity,), row_count, jnp.int32).at[position].set(owners)
    return (slot_table, position.reshape(row_count, top_count))


def routed_exchange(hidden, ids, weights, gate_local, up_local, down_local, capacity):
    experts = lax.axis_size("sp")
    own_count, width = hidden.shape
    top_count = ids.shape[1]
    own_table, positions = slot_layout(ids, experts, capacity)
    padded = jnp.concatenate([hidden, jnp.zeros((1, width), jnp.bfloat16)], axis=0)
    dispatched = padded[own_table].reshape(experts, capacity, width)
    arrived = lax.all_to_all(dispatched, "sp", split_axis=0, concat_axis=0, tiled=True)
    gathered = lax.all_gather(arrived[None], "tp", axis=0, tiled=True)
    activity = expert_activity(gathered.reshape(-1, width), gate_local, up_local)
    expert_out = lax.psum_scatter(
        matmul(activity, down_local).astype(jnp.bfloat16), "tp", scatter_dimension=0, tiled=True
    )
    expert_out = expert_out.reshape(experts, capacity, width)
    returned = lax.all_to_all(expert_out, "sp", split_axis=0, concat_axis=0, tiled=True)
    picked = returned.reshape(experts * capacity, width)[positions.reshape(-1)]
    picked = picked.reshape(own_count, top_count, width)
    return jnp.einsum("tk,tkd->td", weights, picked.astype(jnp.float32))


def shards(
    glu_value,
    glu_gate,
    conv_kernel,
    norm_gain,
    mix_weight,
    residual,
    resid_gain,
    expert_ids,
    route_weight,
    w_gate,
    w_up,
    w_down,
    out_gain,
):
    convolved, head, stats, gains, weights = convolve(glu_value, glu_gate, conv_kernel, norm_gain, mix_weight)
    mixed_rows = scattered_product(convolved, head, stats, gains, weights)
    vmem = pl.BlockSpec(memory_space=pltpu.VMEM)
    hidden = pl.pallas_call(
        hidden_kernel,
        out_shape=jax.ShapeDtypeStruct(residual.shape, jnp.bfloat16),
        in_specs=[vmem] * 5,
        out_specs=vmem,
        compiler_params=pltpu.CompilerParams(vmem_limit_bytes=8 * 2**20),
        name="hidden",
    )(residual, *mixed_rows, resid_gain[None])
    experts = lax.axis_size("sp")
    own_count, top_count = expert_ids.shape
    capacity = 2 * own_count * top_count // experts
    whole_rows = (experts // 2 - 1) * own_count + experts // 2 * capacity
    padded_rows = (experts - 1) * capacity
    ring = lax.axis_size("tp") == 4 and whole_rows <= 2 * padded_rows
    route = routed_ring if ring else routed_exchange
    routed_sum = route(hidden, expert_ids, route_weight, w_gate[0], w_up[0], w_down[0], capacity)
    return normalize(hidden.astype(jnp.float32) + routed_sum, out_gain).astype(jnp.bfloat16)


def solution(mesh):
    in_specs = (
        P("sp", "tp"),
        P("sp", "tp"),
        P(None, "tp"),
        P("tp"),
        P("tp", None),
        P(("sp", "tp"), None),
        P(),
        P(("sp", "tp"), None),
        P(("sp", "tp"), None),
        P("sp", None, "tp"),
        P("sp", None, "tp"),
        P("sp", "tp", None),
        P(),
    )
    out_specs = P(("sp", "tp"), None)
    return jax.shard_map(shards, mesh=mesh, in_specs=in_specs, out_specs=out_specs, check_vma=False)
```

```python
import jax
import jax.numpy as jnp
from jax import lax
from jax.experimental import pallas as pl
from jax.experimental.pallas import tpu as pltpu
from jax.sharding import PartitionSpec as P


EPSILON = 1e-05
LIMIT = 7.0
SLOPE = 1.702


def shifted(block, axis, distance):
    devices = range(lax.axis_size(axis))
    route = [(i - distance, i) for i in devices if i - distance in devices]
    return lax.ppermute(block, axis, route)


def swapped(block, axis, bit):
    return lax.ppermute(block, axis, [(i, i ^ bit) for i in range(lax.axis_size(axis))])


def folded_ring(length):
    return list(range(0, length, 2)) + list(range(1, length, 2))[::-1]


def around(block, distance):
    count = lax.axis_size("sp")
    order = folded_ring(count // 2)
    route = []
    for place, line in enumerate(order):
        target = order[(place + distance) % len(order)]
        route += [(2 * line, 2 * target), (2 * line + 1, 2 * target + 1)]
    return lax.ppermute(block, "sp", route)


def normalize(values, gain_vector):
    centre = jnp.mean(values, axis=-1, keepdims=True)
    spread = jnp.mean(jnp.square(values - centre), axis=-1, keepdims=True)
    return (values - centre) * lax.rsqrt(spread + EPSILON) * gain_vector


def matmul(a, b):
    return jnp.dot(a, b, preferred_element_type=jnp.float32)


def expert_activity(tokens, gate_matrix, up_matrix):
    gated = jnp.minimum(matmul(tokens, gate_matrix), LIMIT)
    upper = jnp.clip(matmul(tokens, up_matrix), -LIMIT, LIMIT)
    return ((upper + 1.0) * gated * jax.nn.sigmoid(SLOPE * gated)).astype(jnp.bfloat16)


def expert_kernel(tokens, gate_matrix, up_matrix, down_matrix, *outs):
    gated = jnp.minimum(matmul(tokens[...], gate_matrix[...]), LIMIT)
    upper = jnp.clip(matmul(tokens[...], up_matrix[...]), -LIMIT, LIMIT)
    activity = (upper + 1.0) * gated / (1.0 + jnp.exp(-SLOPE * gated))
    sums = matmul(activity.astype(jnp.bfloat16), down_matrix[...])
    rows = sums.shape[0] // len(outs)
    for i, out in enumerate(outs):
        out[...] = sums[i * rows : (i + 1) * rows].astype(out.dtype)


def expert_step(tokens, gate_matrix, up_matrix, down_matrix, dtype, parts):
    rows, width = tokens.shape
    vmem = pl.BlockSpec(memory_space=pltpu.VMEM)
    return pl.pallas_call(
        expert_kernel,
        out_shape=(jax.ShapeDtypeStruct((rows // parts, width), dtype),) * parts,
        in_specs=[vmem] * 4,
        out_specs=(vmem,) * parts,
        compiler_params=pltpu.CompilerParams(vmem_limit_bytes=16 * 2**20),
        cost_estimate=pl.CostEstimate(
            flops=6 * rows * width * gate_matrix.shape[1], transcendentals=0, bytes_accessed=0
        ),
        name="expert_step",
    )(tokens, gate_matrix, up_matrix, down_matrix)


def gated_rows(value, gate):
    return (value.astype(jnp.float32) * jax.nn.sigmoid(gate.astype(jnp.float32))).astype(jnp.bfloat16)


def convolve_rows(extended, taps, first, row, rows, window):
    lanes = window.stop - window.start
    sums = jnp.zeros((rows, lanes), jnp.float32)
    for shift in range(8):
        part = jnp.zeros(((rows + 8) // 8, 8, lanes), jnp.float32)
        for k in range(taps.shape[0]):
            if (first + k) % 8 == shift:
                block = extended[pl.ds(row + first + k - shift, rows + 8), window]
                tap = jnp.broadcast_to(taps[k : k + 1, window], (8, lanes))
                part = part + block.reshape(part.shape) * tap[None]
        sums = sums + part.reshape(rows + 8, lanes)[shift : shift + rows]
    return sums


def convolve_kernel(gated, kernel, gain, out, total, squares, taps, gains, extended, arrived, *, pad, rows):
    length, channels = gated.shape
    moves = [
        pltpu.make_async_copy(source, target, arrived.at[i])
        for i, (source, target) in enumerate(((kernel, taps), (gain, gains)))
    ]
    for move in moves:
        move.start()
    extended[pl.ds(0, pad), :] = jnp.zeros((pad, channels), jnp.float32)
    extended[pl.ds(pad, length), :] = gated[...].astype(jnp.float32)
    moves[0].wait()
    first = pad - (taps.shape[0] - 1)

    def body(i, carry):
        row = pl.multiple_of(i * rows, rows)
        own_total = jnp.zeros((rows, 128), jnp.float32)
        own_squares = jnp.zeros((rows, 128), jnp.float32)
        for lane in range(0, channels, 128):
            window = slice(lane, lane + 128)
            sums = convolve_rows(extended, taps, first, row, rows, window)
            out[pl.ds(row, rows), window] = sums
            own_total = own_total + sums
            own_squares = own_squares + sums * sums
        total[pl.ds(row, rows), :] = own_total
        squares[pl.ds(row, rows), :] = own_squares
        return carry

    lax.fori_loop(0, length // rows, body, 0)
    moves[1].wait()


def head_kernel(before, gated, taps, total, squares, head, stats, extended):
    pad, channels = before.shape
    first = pad - (taps.shape[0] - 1)
    extended[0:pad, :] = before[...].astype(jnp.float32)
    extended[pad : 2 * pad, :] = gated[0:pad, :].astype(jnp.float32)
    total[0:pad, :] = jnp.zeros((pad, 128), jnp.float32)
    squares[0:pad, :] = jnp.zeros((pad, 128), jnp.float32)
    for lane in range(0, channels, 128):
        window = slice(lane, lane + 128)
        sums = convolve_rows(extended, taps, first, 0, pad, window)
        head[:, window] = sums
        total[0:pad, :] += sums
        squares[0:pad, :] += sums * sums
    ones = jnp.ones((8, 128), jnp.float32)
    for place, partial in enumerate((total, squares)):
        sums = lax.dot_general(
            ones,
            partial[...],
            (((1,), (1,)), ((), ())),
            precision=lax.Precision.HIGHEST,
            preferred_element_type=jnp.float32,
        )
        stats[place : place + 1, :] = sums[:1]


def in_vmem(*arrays):
    return tuple(pltpu.with_memory_space_constraint(a, pltpu.VMEM) for a in arrays)


def convolve(glu_value, glu_gate, conv_kernel, norm_gain):
    length, channels = glu_value.shape
    rows = min(128, length)
    pad = -(-(conv_kernel.shape[0] - 1) // 16) * 16
    tail = slice(length - pad, length)
    before_rows = shifted(gated_rows(glu_value[tail], glu_gate[tail]), "sp", 1)
    gated = gated_rows(glu_value, glu_gate)
    norm_gain = norm_gain[None]
    vmem, hbm = pl.BlockSpec(memory_space=pltpu.VMEM), pl.BlockSpec(memory_space=pltpu.HBM)
    convolved, total, squares, taps, gains = pl.pallas_call(
        lambda *refs: convolve_kernel(*refs, pad=pad, rows=rows),
        out_shape=(
            jax.ShapeDtypeStruct((length, channels), jnp.float32),
            pltpu.VMEM((length, 128), jnp.float32),
            pltpu.VMEM((length, 128), jnp.float32),
            pltpu.VMEM(conv_kernel.shape, jnp.float32),
            pltpu.VMEM(norm_gain.shape, jnp.float32),
        ),
        in_specs=[vmem, hbm, hbm],
        out_specs=(vmem,) * 5,
        scratch_shapes=[
            pltpu.VMEM((length + pad + 8, channels), jnp.float32),
            pltpu.SemaphoreType.DMA((2,)),
        ],
        compiler_params=pltpu.CompilerParams(vmem_limit_bytes=16 * 2**20),
        name="convolve",
    )(*in_vmem(gated), *(pltpu.with_memory_space_constraint(a, pltpu.HBM) for a in (conv_kernel, norm_gain)))
    head, own = pl.pallas_call(
        head_kernel,
        out_shape=(pltpu.VMEM((pad, channels), jnp.float32), pltpu.VMEM((2, length), jnp.float32)),
        in_specs=[vmem] * 5,
        out_specs=(vmem,) * 2,
        scratch_shapes=[pltpu.VMEM((2 * pad + 8, channels), jnp.float32)],
        compiler_params=pltpu.CompilerParams(vmem_limit_bytes=8 * 2**20),
        name="head",
    )(*in_vmem(before_rows, gated, taps, total, squares))
    stats = [own] + [swapped(own, "tp", d) for d in range(1, lax.axis_size("tp"))]
    return convolved, head, stats, gains


def first_products_kernel(here, convolved, head, gain, weight, *refs, bit, far, shares):
    stats, (mix_in, send, keep, wide, mix_weight, arrived) = refs[:shares], refs[shares:]
    fetch = pltpu.make_async_copy(weight, mix_weight, arrived)
    fetch.start()
    rows, channels = send.shape[0], convolved.shape[1] * shares
    sums = stats[0][...]
    for share in stats[1:]:
        sums = sums + share[...]
    centre = sums[0:1] / channels
    spread = sums[1:2] / channels - centre * centre
    wide[...] = jnp.zeros_like(wide)
    wide[0:1, :] = centre
    wide[1:2, :] = lax.rsqrt(spread + EPSILON)
    place = lax.broadcasted_iota(jnp.int32, (wide.shape[0], 128), 0)
    centre, scale = (
        lax.dot_general(
            wide[...],
            (place == i).astype(jnp.float32),
            (((0,), (0,)), ((), ())),
            precision=lax.Precision.HIGHEST,
            preferred_element_type=jnp.float32,
        )
        for i in (0, 1)
    )
    for lane in range(0, convolved.shape[1], 128):
        window = slice(lane, lane + 128)
        values = jnp.concatenate([head[:, window], convolved[head.shape[0] :, window]], axis=0)
        normed = (values - centre) * scale * gain[:, window]
        mix_in[:, window] = (normed / (1.0 + jnp.exp(-normed))).astype(jnp.bfloat16)
    fetch.wait()
    for d, out in ((far + bit, send), (far, keep)):
        own = mix_in[pl.ds(pl.multiple_of((here[0] ^ d) * rows, rows), rows), :]
        out[...] = matmul(own, mix_weight[...]).astype(out.dtype)


def last_products_kernel(here, mix_in, weight, send, keep, mix_weight, arrived, *, bit):
    fetch = pltpu.make_async_copy(weight, mix_weight, arrived)
    fetch.start()
    fetch.wait()
    rows = send.shape[0]
    for d, out in ((bit, send), (0, keep)):
        own = mix_in[pl.ds(pl.multiple_of((here[0] ^ d) * rows, rows), rows), :]
        out[...] = matmul(own, mix_weight[...]).astype(out.dtype)


def scattered_product(convolved, head, stats, norm_gain, mix_weight):
    count = lax.axis_size("tp")
    assert count == 4
    rows, width = convolved.shape[0] // count, mix_weight.shape[1]
    here = lax.axis_index("tp").reshape(1).astype(jnp.int32)
    vmem, smem = pl.BlockSpec(memory_space=pltpu.VMEM), pl.BlockSpec(memory_space=pltpu.SMEM)
    hbm = pl.BlockSpec(memory_space=pltpu.HBM)
    mix_weight = pltpu.with_memory_space_constraint(mix_weight, pltpu.HBM)
    fetched = [pltpu.VMEM(mix_weight.shape, mix_weight.dtype), pltpu.SemaphoreType.DMA]
    products = (pltpu.VMEM((rows, width), jnp.bfloat16), pltpu.VMEM((rows, width), jnp.float32))
    params = pltpu.CompilerParams(vmem_limit_bytes=8 * 2**20)
    mix_in, far_send, far_keep = pl.pallas_call(
        lambda *refs: first_products_kernel(*refs, bit=1, far=2, shares=count),
        out_shape=(pltpu.VMEM(convolved.shape, jnp.bfloat16),) + products,
        in_specs=[smem] + [vmem] * 3 + [hbm] + [vmem] * count,
        out_specs=(vmem,) * 3,
        scratch_shapes=[pltpu.VMEM((8, convolved.shape[0]), jnp.float32)] + fetched,
        compiler_params=params,
        name="first_products",
    )(here, *in_vmem(convolved, head, norm_gain), mix_weight, *in_vmem(*stats))
    arrived = swapped(far_send, "tp", 1)
    far_sum = (far_keep + arrived.astype(jnp.float32)).astype(jnp.bfloat16)
    from_chip = swapped(far_sum, "tp", 2)
    near_send, near_keep = pl.pallas_call(
        lambda *refs: last_products_kernel(*refs, bit=1),
        out_shape=products,
        in_specs=[smem, vmem, hbm],
        out_specs=(vmem,) * 2,
        scratch_shapes=fetched,
        compiler_params=params,
        name="last_products",
    )(here, *in_vmem(mix_in), mix_weight)
    arrived = swapped(near_send, "tp", 1)
    return near_keep, arrived, from_chip


def hidden_kernel(residual, keep, from_core, from_chip, gain, out):
    values = residual[...].astype(jnp.float32) + keep[...]
    values = values + from_core[...].astype(jnp.float32) + from_chip[...].astype(jnp.float32)
    out[...] = normalize(values, gain[...]).astype(out.dtype)


def blended_kernel(hidden, own_share, carried, gain, out):
    values = hidden[...].astype(jnp.float32) + (own_share[...] + carried[...].astype(jnp.float32))
    out[...] = normalize(values, gain[...]).astype(out.dtype)


def slots_of(ids, weights, expert, capacity):
    named = (ids == expert).astype(jnp.float32)
    chosen = jnp.sum(named, axis=1)
    count = ids.shape[0]
    earlier = (
        lax.broadcasted_iota(jnp.int32, (count, count), 0)
        > lax.broadcasted_iota(jnp.int32, (count, count), 1)
    ).astype(jnp.float32)
    rank = jnp.sum(earlier * chosen[None, :], axis=1)
    places = lax.broadcasted_iota(jnp.int32, (count, capacity), 1).astype(jnp.float32)
    onehot = ((places == rank[:, None]) & (chosen[:, None] > 0)).astype(jnp.bfloat16)
    return onehot, jnp.sum(named * weights, axis=1)


def routed_ring(hidden, ids, weights, gate_local, up_local, down_local, out_gain, capacity):
    steps = lax.axis_size("sp") // 2
    here = lax.axis_index("sp").astype(jnp.float32)
    other = (lax.axis_index("sp") ^ 1).astype(jnp.float32)
    top = ids.shape[1]
    table = jnp.concatenate([ids.astype(jnp.float32), weights], axis=1)
    tables = [table]
    for s in range(1, steps):
        tables.append(around(table, s))
    block = hidden
    carried = None
    for s in range(steps):
        if s + 1 < steps:
            following = around(block, 1)
        own_hot, own_weight = slots_of(tables[s][:, :top], tables[s][:, top:], here, capacity)
        far_hot, far_weight = slots_of(tables[s][:, :top], tables[s][:, top:], other, capacity)
        far_rows = matmul(far_hot.T, block).astype(jnp.bfloat16)
        arrived = swapped(far_rows, "sp", 1)
        picked = matmul(own_hot.T, block).astype(jnp.bfloat16)
        own_x = swapped(picked, "tp", 2)
        far_x = swapped(arrived, "tp", 2)
        near = jnp.concatenate([arrived, far_x, picked, own_x], axis=0)
        far = swapped(near, "tp", 1)
        near_sums = expert_step(near, gate_local, up_local, down_local, jnp.float32, 4)
        far_sums = expert_step(far, gate_local, up_local, down_local, jnp.bfloat16, 2)

        def crossed(send, leave):
            from_core = swapped(send, "tp", 1)
            leave = leave + from_core[capacity:].astype(jnp.float32)
            return from_core[:capacity], swapped(leave.astype(jnp.bfloat16), "tp", 2)

        def summed(keep, from_core, from_chip):
            total = keep + from_core.astype(jnp.float32) + from_chip.astype(jnp.float32)
            return total.astype(jnp.bfloat16)

        theirs = crossed(far_sums[0], near_sums[1])
        mine = crossed(far_sums[1], near_sums[3])
        far_sum = swapped(summed(near_sums[0], *theirs), "sp", 1)
        own_sum = summed(near_sums[2], *mine)
        share = own_weight[:, None] * matmul(own_hot, own_sum) + far_weight[:, None] * matmul(far_hot, far_sum)
        if s == 0:
            own_share = share
        else:
            share = (share if carried is None else carried.astype(jnp.float32) + share).astype(jnp.bfloat16)
        if s:
            carried = around(share, 1)
        block = following
    vmem = pl.BlockSpec(memory_space=pltpu.VMEM)
    return pl.pallas_call(
        blended_kernel,
        out_shape=jax.ShapeDtypeStruct(hidden.shape, jnp.bfloat16),
        in_specs=[vmem] * 4,
        out_specs=vmem,
        compiler_params=pltpu.CompilerParams(vmem_limit_bytes=8 * 2**20),
        name="blended",
    )(*in_vmem(hidden, own_share, carried, out_gain[None]))


def slot_layout(route_ids, experts, capacity):
    row_count, top_count = route_ids.shape
    flat_ids = route_ids.reshape(row_count * top_count)
    onehot = (flat_ids[:, None] == jnp.arange(experts, dtype=jnp.int32)[None, :]).astype(jnp.int32)
    before = jnp.cumsum(onehot, axis=0) - onehot
    slot_rank = jnp.sum(before * onehot, axis=1)
    position = flat_ids * capacity + slot_rank
    owners = jnp.arange(row_count * top_count, dtype=jnp.int32) // top_count
    slot_table = jnp.full((experts * capacity,), row_count, jnp.int32).at[position].set(owners)
    return (slot_table, position.reshape(row_count, top_count))


def routed_exchange(hidden, ids, weights, gate_local, up_local, down_local, out_gain, capacity):
    experts = lax.axis_size("sp")
    own_count, width = hidden.shape
    top_count = ids.shape[1]
    own_table, positions = slot_layout(ids, experts, capacity)
    padded = jnp.concatenate([hidden, jnp.zeros((1, width), jnp.bfloat16)], axis=0)
    dispatched = padded[own_table].reshape(experts, capacity, width)
    arrived = lax.all_to_all(dispatched, "sp", split_axis=0, concat_axis=0, tiled=True)
    gathered = lax.all_gather(arrived[None], "tp", axis=0, tiled=True)
    activity = expert_activity(gathered.reshape(-1, width), gate_local, up_local)
    expert_out = lax.psum_scatter(
        matmul(activity, down_local).astype(jnp.bfloat16), "tp", scatter_dimension=0, tiled=True
    )
    expert_out = expert_out.reshape(experts, capacity, width)
    returned = lax.all_to_all(expert_out, "sp", split_axis=0, concat_axis=0, tiled=True)
    picked = returned.reshape(experts * capacity, width)[positions.reshape(-1)]
    picked = picked.reshape(own_count, top_count, width)
    routed_sum = jnp.einsum("tk,tkd->td", weights, picked.astype(jnp.float32))
    return normalize(hidden.astype(jnp.float32) + routed_sum, out_gain).astype(jnp.bfloat16)


def shards(
    glu_value,
    glu_gate,
    conv_kernel,
    norm_gain,
    mix_weight,
    residual,
    resid_gain,
    expert_ids,
    route_weight,
    w_gate,
    w_up,
    w_down,
    out_gain,
):
    convolved, head, stats, gains = convolve(glu_value, glu_gate, conv_kernel, norm_gain)
    mixed_rows = scattered_product(convolved, head, stats, gains, mix_weight)
    vmem = pl.BlockSpec(memory_space=pltpu.VMEM)
    hidden = pl.pallas_call(
        hidden_kernel,
        out_shape=jax.ShapeDtypeStruct(residual.shape, jnp.bfloat16),
        in_specs=[vmem] * 5,
        out_specs=vmem,
        compiler_params=pltpu.CompilerParams(vmem_limit_bytes=8 * 2**20),
        name="hidden",
    )(residual, *mixed_rows, resid_gain[None])
    experts = lax.axis_size("sp")
    own_count, top_count = expert_ids.shape
    capacity = 2 * own_count * top_count // experts
    whole_rows = (experts // 2 - 1) * own_count + experts // 2 * capacity
    padded_rows = (experts - 1) * capacity
    ring = lax.axis_size("tp") == 4 and whole_rows <= 2 * padded_rows
    route = routed_ring if ring else routed_exchange
    return route(hidden, expert_ids, route_weight, w_gate[0], w_up[0], w_down[0], out_gain, capacity)


def solution(mesh):
    in_specs = (
        P("sp", "tp"),
        P("sp", "tp"),
        P(None, "tp"),
        P("tp"),
        P("tp", None),
        P(("sp", "tp"), None),
        P(),
        P(("sp", "tp"), None),
        P(("sp", "tp"), None),
        P("sp", None, "tp"),
        P("sp", None, "tp"),
        P("sp", "tp", None),
        P(),
    )
    out_specs = P(("sp", "tp"), None)
    return jax.shard_map(shards, mesh=mesh, in_specs=in_specs, out_specs=out_specs, check_vma=False)
```

```python
import jax
import jax.numpy as jnp
from jax import lax
from jax.experimental import pallas as pl
from jax.experimental.pallas import tpu as pltpu
from jax.sharding import PartitionSpec as P


EPSILON = 1e-05
LIMIT = 7.0
SLOPE = 1.702


def shifted(block, axis, distance):
    devices = range(lax.axis_size(axis))
    route = [(i - distance, i) for i in devices if i - distance in devices]
    return lax.ppermute(block, axis, route)


def swapped(block, axis, bit):
    return lax.ppermute(block, axis, [(i, i ^ bit) for i in range(lax.axis_size(axis))])


def folded_ring(length):
    return list(range(0, length, 2)) + list(range(1, length, 2))[::-1]


def around(block, distance):
    count = lax.axis_size("sp")
    order = folded_ring(count // 2)
    route = []
    for place, line in enumerate(order):
        target = order[(place + distance) % len(order)]
        route += [(2 * line, 2 * target), (2 * line + 1, 2 * target + 1)]
    return lax.ppermute(block, "sp", route)


def normalize(values, gain_vector):
    centre = jnp.mean(values, axis=-1, keepdims=True)
    spread = jnp.mean(jnp.square(values - centre), axis=-1, keepdims=True)
    return (values - centre) * lax.rsqrt(spread + EPSILON) * gain_vector


def matmul(a, b):
    return jnp.dot(a, b, preferred_element_type=jnp.float32)


def expert_activity(tokens, gate_matrix, up_matrix):
    gated = jnp.minimum(matmul(tokens, gate_matrix), LIMIT)
    upper = jnp.clip(matmul(tokens, up_matrix), -LIMIT, LIMIT)
    return ((upper + 1.0) * gated * jax.nn.sigmoid(SLOPE * gated)).astype(jnp.bfloat16)


def expert_kernel(tokens, gate_matrix, up_matrix, down_matrix, *outs):
    gated = jnp.minimum(matmul(tokens[...], gate_matrix[...]), LIMIT)
    upper = jnp.clip(matmul(tokens[...], up_matrix[...]), -LIMIT, LIMIT)
    activity = (upper + 1.0) * gated / (1.0 + jnp.exp(-SLOPE * gated))
    sums = matmul(activity.astype(jnp.bfloat16), down_matrix[...])
    rows = sums.shape[0] // len(outs)
    for i, out in enumerate(outs):
        out[...] = sums[i * rows : (i + 1) * rows].astype(out.dtype)


def expert_step(tokens, gate_matrix, up_matrix, down_matrix, dtype, parts):
    rows, width = tokens.shape
    vmem = pl.BlockSpec(memory_space=pltpu.VMEM)
    return pl.pallas_call(
        expert_kernel,
        out_shape=(jax.ShapeDtypeStruct((rows // parts, width), dtype),) * parts,
        in_specs=[vmem] * 4,
        out_specs=(vmem,) * parts,
        compiler_params=pltpu.CompilerParams(vmem_limit_bytes=16 * 2**20),
        cost_estimate=pl.CostEstimate(
            flops=6 * rows * width * gate_matrix.shape[1], transcendentals=0, bytes_accessed=0
        ),
        name="expert",
    )(tokens, gate_matrix, up_matrix, down_matrix)


def gated_rows(value, gate):
    return (value.astype(jnp.float32) * jax.nn.sigmoid(gate.astype(jnp.float32))).astype(jnp.bfloat16)


def convolve_rows(extended, taps, first, row, rows, window):
    lanes = window.stop - window.start
    sums = jnp.zeros((rows, lanes), jnp.float32)
    for shift in range(8):
        part = jnp.zeros(((rows + 8) // 8, 8, lanes), jnp.float32)
        for k in range(taps.shape[0]):
            if (first + k) % 8 == shift:
                block = extended[pl.ds(row + first + k - shift, rows + 8), window]
                tap = jnp.broadcast_to(taps[k : k + 1, window], (8, lanes))
                part = part + block.reshape(part.shape) * tap[None]
        sums = sums + part.reshape(rows + 8, lanes)[shift : shift + rows]
    return sums


def convolve_kernel(gated, kernel, gain, out, total, squares, taps, gains, extended, arrived, *, pad, rows):
    length, channels = gated.shape
    moves = [
        pltpu.make_async_copy(source, target, arrived.at[i])
        for i, (source, target) in enumerate(((kernel, taps), (gain, gains)))
    ]
    for move in moves:
        move.start()
    extended[pl.ds(0, pad), :] = jnp.zeros((pad, channels), jnp.float32)
    extended[pl.ds(pad, length), :] = gated[...].astype(jnp.float32)
    moves[0].wait()
    first = pad - (taps.shape[0] - 1)

    def body(i, carry):
        row = pl.multiple_of(i * rows, rows)
        own_total = jnp.zeros((rows, 128), jnp.float32)
        own_squares = jnp.zeros((rows, 128), jnp.float32)
        for lane in range(0, channels, 128):
            window = slice(lane, lane + 128)
            sums = convolve_rows(extended, taps, first, row, rows, window)
            out[pl.ds(row, rows), window] = sums
            own_total = own_total + sums
            own_squares = own_squares + sums * sums
        total[pl.ds(row, rows), :] = own_total
        squares[pl.ds(row, rows), :] = own_squares
        return carry

    lax.fori_loop(0, length // rows, body, 0)
    moves[1].wait()


def head_kernel(before, gated, taps, total, squares, head, stats, extended):
    pad, channels = before.shape
    first = pad - (taps.shape[0] - 1)
    extended[0:pad, :] = before[...].astype(jnp.float32)
    extended[pad : 2 * pad, :] = gated[0:pad, :].astype(jnp.float32)
    total[0:pad, :] = jnp.zeros((pad, 128), jnp.float32)
    squares[0:pad, :] = jnp.zeros((pad, 128), jnp.float32)
    for lane in range(0, channels, 128):
        window = slice(lane, lane + 128)
        sums = convolve_rows(extended, taps, first, 0, pad, window)
        head[:, window] = sums
        total[0:pad, :] += sums
        squares[0:pad, :] += sums * sums
    ones = jnp.ones((8, 128), jnp.float32)
    for place, partial in enumerate((total, squares)):
        sums = lax.dot_general(
            ones,
            partial[...],
            (((1,), (1,)), ((), ())),
            precision=lax.Precision.HIGHEST,
            preferred_element_type=jnp.float32,
        )
        stats[place : place + 1, :] = sums[:1]


def in_vmem(*arrays):
    return tuple(pltpu.with_memory_space_constraint(a, pltpu.VMEM) for a in arrays)


def convolve(glu_value, glu_gate, conv_kernel, norm_gain):
    length, channels = glu_value.shape
    rows = min(128, length)
    pad = -(-(conv_kernel.shape[0] - 1) // 16) * 16
    tail = slice(length - pad, length)
    before_rows = shifted(gated_rows(glu_value[tail], glu_gate[tail]), "sp", 1)
    gated = gated_rows(glu_value, glu_gate)
    norm_gain = norm_gain[None]
    vmem, hbm = pl.BlockSpec(memory_space=pltpu.VMEM), pl.BlockSpec(memory_space=pltpu.HBM)
    convolved, total, squares, taps, gains = pl.pallas_call(
        lambda *refs: convolve_kernel(*refs, pad=pad, rows=rows),
        out_shape=(
            jax.ShapeDtypeStruct((length, channels), jnp.float32),
            pltpu.VMEM((length, 128), jnp.float32),
            pltpu.VMEM((length, 128), jnp.float32),
            pltpu.VMEM(conv_kernel.shape, jnp.float32),
            pltpu.VMEM(norm_gain.shape, jnp.float32),
        ),
        in_specs=[vmem, hbm, hbm],
        out_specs=(vmem,) * 5,
        scratch_shapes=[
            pltpu.VMEM((length + pad + 8, channels), jnp.float32),
            pltpu.SemaphoreType.DMA((2,)),
        ],
        compiler_params=pltpu.CompilerParams(vmem_limit_bytes=16 * 2**20),
        name="convolve",
    )(*in_vmem(gated), *(pltpu.with_memory_space_constraint(a, pltpu.HBM) for a in (conv_kernel, norm_gain)))
    head, own = pl.pallas_call(
        head_kernel,
        out_shape=(pltpu.VMEM((pad, channels), jnp.float32), pltpu.VMEM((2, length), jnp.float32)),
        in_specs=[vmem] * 5,
        out_specs=(vmem,) * 2,
        scratch_shapes=[pltpu.VMEM((2 * pad + 8, channels), jnp.float32)],
        compiler_params=pltpu.CompilerParams(vmem_limit_bytes=8 * 2**20),
        name="head",
    )(*in_vmem(before_rows, gated, taps, total, squares))
    stats = [own] + [swapped(own, "tp", d) for d in range(1, lax.axis_size("tp"))]
    return convolved, head, stats, gains


def first_products_kernel(here, convolved, head, gain, weight, *refs, bit, far, shares):
    stats, (mix_in, send, keep, wide, mix_weight, arrived) = refs[:shares], refs[shares:]
    fetch = pltpu.make_async_copy(weight, mix_weight, arrived)
    fetch.start()
    rows, channels = send.shape[0], convolved.shape[1] * shares
    sums = stats[0][...]
    for share in stats[1:]:
        sums = sums + share[...]
    centre = sums[0:1] / channels
    spread = sums[1:2] / channels - centre * centre
    wide[...] = jnp.zeros_like(wide)
    wide[0:1, :] = centre
    wide[1:2, :] = lax.rsqrt(spread + EPSILON)
    place = lax.broadcasted_iota(jnp.int32, (wide.shape[0], 128), 0)
    centre, scale = (
        lax.dot_general(
            wide[...],
            (place == i).astype(jnp.float32),
            (((0,), (0,)), ((), ())),
            precision=lax.Precision.HIGHEST,
            preferred_element_type=jnp.float32,
        )
        for i in (0, 1)
    )
    for lane in range(0, convolved.shape[1], 128):
        window = slice(lane, lane + 128)
        values = jnp.concatenate([head[:, window], convolved[head.shape[0] :, window]], axis=0)
        normed = (values - centre) * scale * gain[:, window]
        mix_in[:, window] = (normed / (1.0 + jnp.exp(-normed))).astype(jnp.bfloat16)
    fetch.wait()
    for d, out in ((far + bit, send), (far, keep)):
        own = mix_in[pl.ds(pl.multiple_of((here[0] ^ d) * rows, rows), rows), :]
        out[...] = matmul(own, mix_weight[...]).astype(out.dtype)


def last_products_kernel(here, mix_in, weight, send, keep, mix_weight, arrived, *, bit):
    fetch = pltpu.make_async_copy(weight, mix_weight, arrived)
    fetch.start()
    fetch.wait()
    rows = send.shape[0]
    for d, out in ((bit, send), (0, keep)):
        own = mix_in[pl.ds(pl.multiple_of((here[0] ^ d) * rows, rows), rows), :]
        out[...] = matmul(own, mix_weight[...]).astype(out.dtype)


def scattered_product(convolved, head, stats, norm_gain, mix_weight):
    count = lax.axis_size("tp")
    assert count == 4
    rows, width = convolved.shape[0] // count, mix_weight.shape[1]
    here = lax.axis_index("tp").reshape(1).astype(jnp.int32)
    vmem, smem = pl.BlockSpec(memory_space=pltpu.VMEM), pl.BlockSpec(memory_space=pltpu.SMEM)
    hbm = pl.BlockSpec(memory_space=pltpu.HBM)
    mix_weight = pltpu.with_memory_space_constraint(mix_weight, pltpu.HBM)
    fetched = [pltpu.VMEM(mix_weight.shape, mix_weight.dtype), pltpu.SemaphoreType.DMA]
    products = (pltpu.VMEM((rows, width), jnp.bfloat16), pltpu.VMEM((rows, width), jnp.float32))
    params = pltpu.CompilerParams(vmem_limit_bytes=8 * 2**20)
    mix_in, far_send, far_keep = pl.pallas_call(
        lambda *refs: first_products_kernel(*refs, bit=1, far=2, shares=count),
        out_shape=(pltpu.VMEM(convolved.shape, jnp.bfloat16),) + products,
        in_specs=[smem] + [vmem] * 3 + [hbm] + [vmem] * count,
        out_specs=(vmem,) * 3,
        scratch_shapes=[pltpu.VMEM((8, convolved.shape[0]), jnp.float32)] + fetched,
        compiler_params=params,
        name="fp",
    )(here, *in_vmem(convolved, head, norm_gain), mix_weight, *in_vmem(*stats))
    arrived = swapped(far_send, "tp", 1)
    far_sum = (far_keep + arrived.astype(jnp.float32)).astype(jnp.bfloat16)
    from_chip = swapped(far_sum, "tp", 2)
    near_send, near_keep = pl.pallas_call(
        lambda *refs: last_products_kernel(*refs, bit=1),
        out_shape=products,
        in_specs=[smem, vmem, hbm],
        out_specs=(vmem,) * 2,
        scratch_shapes=fetched,
        compiler_params=params,
        name="lp",
    )(here, *in_vmem(mix_in), mix_weight)
    arrived = swapped(near_send, "tp", 1)
    return near_keep, arrived, from_chip


def hidden_kernel(residual, keep, from_core, from_chip, gain, out):
    values = residual[...].astype(jnp.float32) + keep[...]
    values = values + from_core[...].astype(jnp.float32) + from_chip[...].astype(jnp.float32)
    out[...] = normalize(values, gain[...]).astype(out.dtype)


def blended_kernel(hidden, own_share, carried, gain, out):
    values = hidden[...].astype(jnp.float32) + (own_share[...] + carried[...].astype(jnp.float32))
    out[...] = normalize(values, gain[...]).astype(out.dtype)


def slots_of(ids, weights, expert, capacity):
    named = (ids == expert).astype(jnp.float32)
    chosen = jnp.sum(named, axis=1)
    count = ids.shape[0]
    earlier = (
        lax.broadcasted_iota(jnp.int32, (count, count), 0)
        > lax.broadcasted_iota(jnp.int32, (count, count), 1)
    ).astype(jnp.float32)
    rank = jnp.sum(earlier * chosen[None, :], axis=1)
    places = lax.broadcasted_iota(jnp.int32, (count, capacity), 1).astype(jnp.float32)
    onehot = ((places == rank[:, None]) & (chosen[:, None] > 0)).astype(jnp.bfloat16)
    return onehot, jnp.sum(named * weights, axis=1)


def routed_ring(hidden, ids, weights, gate_local, up_local, down_local, out_gain, capacity):
    steps = lax.axis_size("sp") // 2
    here = lax.axis_index("sp").astype(jnp.float32)
    other = (lax.axis_index("sp") ^ 1).astype(jnp.float32)
    top = ids.shape[1]
    table = jnp.concatenate([ids.astype(jnp.float32), weights], axis=1)
    tables = [table]
    for s in range(1, steps):
        tables.append(around(table, s))
    block = hidden
    carried = None
    for s in range(steps):
        if s + 1 < steps:
            following = around(block, 1)
        own_hot, own_weight = slots_of(tables[s][:, :top], tables[s][:, top:], here, capacity)
        far_hot, far_weight = slots_of(tables[s][:, :top], tables[s][:, top:], other, capacity)
        far_rows = matmul(far_hot.T, block).astype(jnp.bfloat16)
        arrived = swapped(far_rows, "sp", 1)
        picked = matmul(own_hot.T, block).astype(jnp.bfloat16)
        own_x = swapped(picked, "tp", 2)
        far_x = swapped(arrived, "tp", 2)
        near = jnp.concatenate([arrived, far_x, picked, own_x], axis=0)
        far = swapped(near, "tp", 1)
        near_sums = expert_step(near, gate_local, up_local, down_local, jnp.float32, 4)
        far_sums = expert_step(far, gate_local, up_local, down_local, jnp.bfloat16, 2)

        def crossed(send, leave):
            from_core = swapped(send, "tp", 1)
            leave = leave + from_core[capacity:].astype(jnp.float32)
            return from_core[:capacity], swapped(leave.astype(jnp.bfloat16), "tp", 2)

        def summed(keep, from_core, from_chip):
            total = keep + from_core.astype(jnp.float32) + from_chip.astype(jnp.float32)
            return total.astype(jnp.bfloat16)

        theirs = crossed(far_sums[0], near_sums[1])
        mine = crossed(far_sums[1], near_sums[3])
        far_sum = swapped(summed(near_sums[0], *theirs), "sp", 1)
        own_sum = summed(near_sums[2], *mine)
        share = own_weight[:, None] * matmul(own_hot, own_sum) + far_weight[:, None] * matmul(far_hot, far_sum)
        if s == 0:
            own_share = share
        else:
            share = (share if carried is None else carried.astype(jnp.float32) + share).astype(jnp.bfloat16)
        if s:
            carried = around(share, 1)
        block = following
    vmem = pl.BlockSpec(memory_space=pltpu.VMEM)
    return pl.pallas_call(
        blended_kernel,
        out_shape=jax.ShapeDtypeStruct(hidden.shape, jnp.bfloat16),
        in_specs=[vmem] * 4,
        out_specs=vmem,
        compiler_params=pltpu.CompilerParams(vmem_limit_bytes=8 * 2**20),
        name="blended",
    )(*in_vmem(hidden, own_share, carried, out_gain[None]))


def slot_layout(route_ids, experts, capacity):
    row_count, top_count = route_ids.shape
    flat_ids = route_ids.reshape(row_count * top_count)
    onehot = (flat_ids[:, None] == jnp.arange(experts, dtype=jnp.int32)[None, :]).astype(jnp.int32)
    before = jnp.cumsum(onehot, axis=0) - onehot
    slot_rank = jnp.sum(before * onehot, axis=1)
    position = flat_ids * capacity + slot_rank
    owners = jnp.arange(row_count * top_count, dtype=jnp.int32) // top_count
    slot_table = jnp.full((experts * capacity,), row_count, jnp.int32).at[position].set(owners)
    return (slot_table, position.reshape(row_count, top_count))


def routed_exchange(hidden, ids, weights, gate_local, up_local, down_local, out_gain, capacity):
    experts = lax.axis_size("sp")
    own_count, width = hidden.shape
    top_count = ids.shape[1]
    own_table, positions = slot_layout(ids, experts, capacity)
    padded = jnp.concatenate([hidden, jnp.zeros((1, width), jnp.bfloat16)], axis=0)
    dispatched = padded[own_table].reshape(experts, capacity, width)
    arrived = lax.all_to_all(dispatched, "sp", split_axis=0, concat_axis=0, tiled=True)
    gathered = lax.all_gather(arrived[None], "tp", axis=0, tiled=True)
    activity = expert_activity(gathered.reshape(-1, width), gate_local, up_local)
    expert_out = lax.psum_scatter(
        matmul(activity, down_local).astype(jnp.bfloat16), "tp", scatter_dimension=0, tiled=True
    )
    expert_out = expert_out.reshape(experts, capacity, width)
    returned = lax.all_to_all(expert_out, "sp", split_axis=0, concat_axis=0, tiled=True)
    picked = returned.reshape(experts * capacity, width)[positions.reshape(-1)]
    picked = picked.reshape(own_count, top_count, width)
    routed_sum = jnp.einsum("tk,tkd->td", weights, picked.astype(jnp.float32))
    return normalize(hidden.astype(jnp.float32) + routed_sum, out_gain).astype(jnp.bfloat16)


def shards(
    glu_value,
    glu_gate,
    conv_kernel,
    norm_gain,
    mix_weight,
    residual,
    resid_gain,
    expert_ids,
    route_weight,
    w_gate,
    w_up,
    w_down,
    out_gain,
):
    convolved, head, stats, gains = convolve(glu_value, glu_gate, conv_kernel, norm_gain)
    mixed_rows = scattered_product(convolved, head, stats, gains, mix_weight)
    vmem = pl.BlockSpec(memory_space=pltpu.VMEM)
    hidden = pl.pallas_call(
        hidden_kernel,
        out_shape=jax.ShapeDtypeStruct(residual.shape, jnp.bfloat16),
        in_specs=[vmem] * 5,
        out_specs=vmem,
        compiler_params=pltpu.CompilerParams(vmem_limit_bytes=8 * 2**20),
        name="hidden",
    )(residual, *mixed_rows, resid_gain[None])
    experts = lax.axis_size("sp")
    own_count, top_count = expert_ids.shape
    capacity = 2 * own_count * top_count // experts
    whole_rows = (experts // 2 - 1) * own_count + experts // 2 * capacity
    padded_rows = (experts - 1) * capacity
    ring = lax.axis_size("tp") == 4 and whole_rows <= 2 * padded_rows
    route = routed_ring if ring else routed_exchange
    return route(hidden, expert_ids, route_weight, w_gate[0], w_up[0], w_down[0], out_gain, capacity)


def solution(mesh):
    in_specs = (
        P("sp", "tp"),
        P("sp", "tp"),
        P(None, "tp"),
        P("tp"),
        P("tp", None),
        P(("sp", "tp"), None),
        P(),
        P(("sp", "tp"), None),
        P(("sp", "tp"), None),
        P("sp", None, "tp"),
        P("sp", None, "tp"),
        P("sp", "tp", None),
        P(),
    )
    out_specs = P(("sp", "tp"), None)
    return jax.shard_map(shards, mesh=mesh, in_specs=in_specs, out_specs=out_specs, check_vma=False)
```

```python
import jax
import jax.numpy as jnp
from jax import lax
from jax.experimental import pallas as pl
from jax.experimental.pallas import tpu as pltpu
from jax.sharding import PartitionSpec as P


EPSILON = 1e-05
LIMIT = 7.0
SLOPE = 1.702


def shifted(block, axis, distance):
    devices = range(lax.axis_size(axis))
    route = [(i - distance, i) for i in devices if i - distance in devices]
    return lax.ppermute(block, axis, route)


def swapped(block, axis, bit):
    return lax.ppermute(block, axis, [(i, i ^ bit) for i in range(lax.axis_size(axis))])


def folded_ring(length):
    return list(range(0, length, 2)) + list(range(1, length, 2))[::-1]


def around(block, distance):
    count = lax.axis_size("sp")
    order = folded_ring(count // 2)
    route = []
    for place, line in enumerate(order):
        target = order[(place + distance) % len(order)]
        route += [(2 * line, 2 * target), (2 * line + 1, 2 * target + 1)]
    return lax.ppermute(block, "sp", route)


def normalize(values, gain_vector):
    centre = jnp.mean(values, axis=-1, keepdims=True)
    spread = jnp.mean(jnp.square(values - centre), axis=-1, keepdims=True)
    return (values - centre) * lax.rsqrt(spread + EPSILON) * gain_vector


def matmul(a, b):
    return jnp.dot(a, b, preferred_element_type=jnp.float32)


def expert_activity(tokens, gate_matrix, up_matrix):
    gated = jnp.minimum(matmul(tokens, gate_matrix), LIMIT)
    upper = jnp.clip(matmul(tokens, up_matrix), -LIMIT, LIMIT)
    return ((upper + 1.0) * gated * jax.nn.sigmoid(SLOPE * gated)).astype(jnp.bfloat16)


def expert_kernel(tokens, gate_matrix, up_matrix, down_matrix, *outs):
    gated = jnp.minimum(matmul(tokens[...], gate_matrix[...]), LIMIT)
    upper = jnp.clip(matmul(tokens[...], up_matrix[...]), -LIMIT, LIMIT)
    activity = (upper + 1.0) * gated / (1.0 + jnp.exp(-SLOPE * gated))
    sums = matmul(activity.astype(jnp.bfloat16), down_matrix[...])
    rows = sums.shape[0] // len(outs)
    for i, out in enumerate(outs):
        out[...] = sums[i * rows : (i + 1) * rows].astype(out.dtype)


def expert_step(tokens, gate_matrix, up_matrix, down_matrix, dtype, parts):
    rows, width = tokens.shape
    vmem = pl.BlockSpec(memory_space=pltpu.VMEM)
    return pl.pallas_call(
        expert_kernel,
        out_shape=(jax.ShapeDtypeStruct((rows // parts, width), dtype),) * parts,
        in_specs=[vmem] * 4,
        out_specs=(vmem,) * parts,
        compiler_params=pltpu.CompilerParams(vmem_limit_bytes=16 * 2**20),
        cost_estimate=pl.CostEstimate(
            flops=6 * rows * width * gate_matrix.shape[1], transcendentals=0, bytes_accessed=0
        ),
        name="expert",
    )(tokens, gate_matrix, up_matrix, down_matrix)


def gated_rows(value, gate):
    return (value.astype(jnp.float32) * jax.nn.sigmoid(gate.astype(jnp.float32))).astype(jnp.bfloat16)


def convolve_rows(extended, taps, first, row, rows, window):
    lanes = window.stop - window.start
    sums = jnp.zeros((rows, lanes), jnp.float32)
    for shift in range(8):
        part = jnp.zeros(((rows + 8) // 8, 8, lanes), jnp.float32)
        for k in range(taps.shape[0]):
            if (first + k) % 8 == shift:
                block = extended[pl.ds(row + first + k - shift, rows + 8), window]
                tap = jnp.broadcast_to(taps[k : k + 1, window], (8, lanes))
                part = part + block.reshape(part.shape) * tap[None]
        sums = sums + part.reshape(rows + 8, lanes)[shift : shift + rows]
    return sums


def convolve_kernel(gated, kernel, gain, out, total, squares, taps, gains, extended, arrived, *, pad, rows):
    length, channels = gated.shape
    moves = [
        pltpu.make_async_copy(source, target, arrived.at[i])
        for i, (source, target) in enumerate(((kernel, taps), (gain, gains)))
    ]
    for move in moves:
        move.start()
    extended[pl.ds(0, pad), :] = jnp.zeros((pad, channels), jnp.float32)
    extended[pl.ds(pad, length), :] = gated[...].astype(jnp.float32)
    moves[0].wait()
    first = pad - (taps.shape[0] - 1)

    def body(i, carry):
        row = pl.multiple_of(i * rows, rows)
        own_total = jnp.zeros((rows, 128), jnp.float32)
        own_squares = jnp.zeros((rows, 128), jnp.float32)
        for lane in range(0, channels, 128):
            window = slice(lane, lane + 128)
            sums = convolve_rows(extended, taps, first, row, rows, window)
            out[pl.ds(row, rows), window] = sums
            own_total = own_total + sums
            own_squares = own_squares + sums * sums
        total[pl.ds(row, rows), :] = own_total
        squares[pl.ds(row, rows), :] = own_squares
        return carry

    lax.fori_loop(0, length // rows, body, 0)
    moves[1].wait()


def head_kernel(before, gated, taps, total, squares, head, stats, extended):
    pad, channels = before.shape
    first = pad - (taps.shape[0] - 1)
    extended[0:pad, :] = before[...].astype(jnp.float32)
    extended[pad : 2 * pad, :] = gated[0:pad, :].astype(jnp.float32)
    own_total = jnp.zeros((pad, 128), jnp.float32)
    own_squares = jnp.zeros((pad, 128), jnp.float32)
    for lane in range(0, channels, 128):
        window = slice(lane, lane + 128)
        sums = convolve_rows(extended, taps, first, 0, pad, window)
        head[:, window] = sums
        own_total = own_total + sums
        own_squares = own_squares + sums * sums
    ones = jnp.ones((8, 128), jnp.float32)
    for place, (own, partial) in enumerate(((own_total, total), (own_squares, squares))):
        sums = lax.dot_general(
            ones,
            jnp.concatenate([own, partial[pad:, :]], axis=0),
            (((1,), (1,)), ((), ())),
            precision=lax.Precision.HIGHEST,
            preferred_element_type=jnp.float32,
        )
        stats[place : place + 1, :] = sums[:1]


def in_vmem(*arrays):
    return tuple(pltpu.with_memory_space_constraint(a, pltpu.VMEM) for a in arrays)


def convolve(glu_value, glu_gate, conv_kernel, norm_gain):
    length, channels = glu_value.shape
    rows = min(128, length)
    pad = -(-(conv_kernel.shape[0] - 1) // 16) * 16
    tail = slice(length - pad, length)
    before_rows = shifted(gated_rows(glu_value[tail], glu_gate[tail]), "sp", 1)
    gated = gated_rows(glu_value, glu_gate)
    norm_gain = norm_gain[None]
    vmem, hbm = pl.BlockSpec(memory_space=pltpu.VMEM), pl.BlockSpec(memory_space=pltpu.HBM)
    convolved, total, squares, taps, gains = pl.pallas_call(
        lambda *refs: convolve_kernel(*refs, pad=pad, rows=rows),
        out_shape=(
            jax.ShapeDtypeStruct((length, channels), jnp.float32),
            pltpu.VMEM((length, 128), jnp.float32),
            pltpu.VMEM((length, 128), jnp.float32),
            pltpu.VMEM(conv_kernel.shape, jnp.float32),
            pltpu.VMEM(norm_gain.shape, jnp.float32),
        ),
        in_specs=[vmem, hbm, hbm],
        out_specs=(vmem,) * 5,
        scratch_shapes=[
            pltpu.VMEM((length + pad + 8, channels), jnp.float32),
            pltpu.SemaphoreType.DMA((2,)),
        ],
        compiler_params=pltpu.CompilerParams(vmem_limit_bytes=16 * 2**20),
        name="convolve",
    )(*in_vmem(gated), *(pltpu.with_memory_space_constraint(a, pltpu.HBM) for a in (conv_kernel, norm_gain)))
    head, own = pl.pallas_call(
        head_kernel,
        out_shape=(pltpu.VMEM((pad, channels), jnp.float32), pltpu.VMEM((2, length), jnp.float32)),
        in_specs=[vmem] * 5,
        out_specs=(vmem,) * 2,
        scratch_shapes=[pltpu.VMEM((2 * pad + 8, channels), jnp.float32)],
        compiler_params=pltpu.CompilerParams(vmem_limit_bytes=8 * 2**20),
        name="head",
    )(*in_vmem(before_rows, gated, taps, total, squares))
    stats = [own] + [swapped(own, "tp", d) for d in range(1, lax.axis_size("tp"))]
    return convolved, head, stats, gains


def first_products_kernel(here, convolved, head, gain, weight, *refs, bit, far, shares):
    stats, (mix_in, send, keep, wide, mix_weight, arrived) = refs[:shares], refs[shares:]
    fetch = pltpu.make_async_copy(weight, mix_weight, arrived)
    fetch.start()
    rows, channels = send.shape[0], convolved.shape[1] * shares
    sums = stats[0][...]
    for share in stats[1:]:
        sums = sums + share[...]
    centre = sums[0:1] / channels
    spread = sums[1:2] / channels - centre * centre
    wide[...] = jnp.zeros_like(wide)
    wide[0:1, :] = centre
    wide[1:2, :] = lax.rsqrt(spread + EPSILON)
    place = lax.broadcasted_iota(jnp.int32, (wide.shape[0], 128), 0)
    centre, scale = (
        lax.dot_general(
            wide[...],
            (place == i).astype(jnp.float32),
            (((0,), (0,)), ((), ())),
            precision=lax.Precision.HIGHEST,
            preferred_element_type=jnp.float32,
        )
        for i in (0, 1)
    )
    for lane in range(0, convolved.shape[1], 128):
        window = slice(lane, lane + 128)
        values = jnp.concatenate([head[:, window], convolved[head.shape[0] :, window]], axis=0)
        normed = (values - centre) * scale * gain[:, window]
        mix_in[:, window] = (normed / (1.0 + jnp.exp(-normed))).astype(jnp.bfloat16)
    fetch.wait()
    for d, out in ((far + bit, send), (far, keep)):
        own = mix_in[pl.ds(pl.multiple_of((here[0] ^ d) * rows, rows), rows), :]
        out[...] = matmul(own, mix_weight[...]).astype(out.dtype)


def last_products_kernel(here, mix_in, weight, send, keep, mix_weight, arrived, *, bit):
    fetch = pltpu.make_async_copy(weight, mix_weight, arrived)
    fetch.start()
    fetch.wait()
    rows = send.shape[0]
    for d, out in ((bit, send), (0, keep)):
        own = mix_in[pl.ds(pl.multiple_of((here[0] ^ d) * rows, rows), rows), :]
        out[...] = matmul(own, mix_weight[...]).astype(out.dtype)


def scattered_product(convolved, head, stats, norm_gain, mix_weight):
    count = lax.axis_size("tp")
    assert count == 4
    rows, width = convolved.shape[0] // count, mix_weight.shape[1]
    here = lax.axis_index("tp").reshape(1).astype(jnp.int32)
    vmem, smem = pl.BlockSpec(memory_space=pltpu.VMEM), pl.BlockSpec(memory_space=pltpu.SMEM)
    hbm = pl.BlockSpec(memory_space=pltpu.HBM)
    mix_weight = pltpu.with_memory_space_constraint(mix_weight, pltpu.HBM)
    fetched = [pltpu.VMEM(mix_weight.shape, mix_weight.dtype), pltpu.SemaphoreType.DMA]
    products = (pltpu.VMEM((rows, width), jnp.bfloat16), pltpu.VMEM((rows, width), jnp.float32))
    params = pltpu.CompilerParams(vmem_limit_bytes=8 * 2**20)
    mix_in, far_send, far_keep = pl.pallas_call(
        lambda *refs: first_products_kernel(*refs, bit=1, far=2, shares=count),
        out_shape=(pltpu.VMEM(convolved.shape, jnp.bfloat16),) + products,
        in_specs=[smem] + [vmem] * 3 + [hbm] + [vmem] * count,
        out_specs=(vmem,) * 3,
        scratch_shapes=[pltpu.VMEM((8, convolved.shape[0]), jnp.float32)] + fetched,
        compiler_params=params,
        name="fp",
    )(here, *in_vmem(convolved, head, norm_gain), mix_weight, *in_vmem(*stats))
    arrived = swapped(far_send, "tp", 1)
    far_sum = (far_keep + arrived.astype(jnp.float32)).astype(jnp.bfloat16)
    from_chip = swapped(far_sum, "tp", 2)
    near_send, near_keep = pl.pallas_call(
        lambda *refs: last_products_kernel(*refs, bit=1),
        out_shape=products,
        in_specs=[smem, vmem, hbm],
        out_specs=(vmem,) * 2,
        scratch_shapes=fetched,
        compiler_params=params,
        name="lp",
    )(here, *in_vmem(mix_in), mix_weight)
    arrived = swapped(near_send, "tp", 1)
    return near_keep, arrived, from_chip


def hidden_kernel(residual, keep, from_core, from_chip, gain, out):
    values = residual[...].astype(jnp.float32) + keep[...]
    values = values + from_core[...].astype(jnp.float32) + from_chip[...].astype(jnp.float32)
    out[...] = normalize(values, gain[...]).astype(out.dtype)


def blended_kernel(hidden, own_share, carried, gain, out):
    values = hidden[...].astype(jnp.float32) + (own_share[...] + carried[...].astype(jnp.float32))
    out[...] = normalize(values, gain[...]).astype(out.dtype)


def slots_of(ids, weights, expert, capacity):
    named = (ids == expert).astype(jnp.float32)
    chosen = jnp.sum(named, axis=1)
    count = ids.shape[0]
    earlier = (
        lax.broadcasted_iota(jnp.int32, (count, count), 0)
        > lax.broadcasted_iota(jnp.int32, (count, count), 1)
    ).astype(jnp.float32)
    rank = jnp.sum(earlier * chosen[None, :], axis=1)
    places = lax.broadcasted_iota(jnp.int32, (count, capacity), 1).astype(jnp.float32)
    onehot = ((places == rank[:, None]) & (chosen[:, None] > 0)).astype(jnp.bfloat16)
    return onehot, jnp.sum(named * weights, axis=1)


def routed_ring(hidden, ids, weights, gate_local, up_local, down_local, out_gain, capacity):
    steps = lax.axis_size("sp") // 2
    here = lax.axis_index("sp").astype(jnp.float32)
    other = (lax.axis_index("sp") ^ 1).astype(jnp.float32)
    top = ids.shape[1]
    table = jnp.concatenate([ids.astype(jnp.float32), weights], axis=1)
    tables = [table]
    for s in range(1, steps):
        tables.append(around(table, s))
    block = hidden
    carried = None
    for s in range(steps):
        if s + 1 < steps:
            following = around(block, 1)
        own_hot, own_weight = slots_of(tables[s][:, :top], tables[s][:, top:], here, capacity)
        far_hot, far_weight = slots_of(tables[s][:, :top], tables[s][:, top:], other, capacity)
        far_rows = matmul(far_hot.T, block).astype(jnp.bfloat16)
        arrived = swapped(far_rows, "sp", 1)
        picked = matmul(own_hot.T, block).astype(jnp.bfloat16)
        own_x = swapped(picked, "tp", 2)
        far_x = swapped(arrived, "tp", 2)
        near = jnp.concatenate([arrived, far_x, picked, own_x], axis=0)
        far = swapped(near, "tp", 1)
        near_sums = expert_step(near, gate_local, up_local, down_local, jnp.float32, 4)
        far_sums = expert_step(far, gate_local, up_local, down_local, jnp.bfloat16, 2)

        def crossed(send, leave):
            from_core = swapped(send, "tp", 1)
            leave = leave + from_core[capacity:].astype(jnp.float32)
            return from_core[:capacity], swapped(leave.astype(jnp.bfloat16), "tp", 2)

        def summed(keep, from_core, from_chip):
            total = keep + from_core.astype(jnp.float32) + from_chip.astype(jnp.float32)
            return total.astype(jnp.bfloat16)

        theirs = crossed(far_sums[0], near_sums[1])
        mine = crossed(far_sums[1], near_sums[3])
        far_sum = swapped(summed(near_sums[0], *theirs), "sp", 1)
        own_sum = summed(near_sums[2], *mine)
        share = own_weight[:, None] * matmul(own_hot, own_sum) + far_weight[:, None] * matmul(far_hot, far_sum)
        if s == 0:
            own_share = share
        else:
            share = (share if carried is None else carried.astype(jnp.float32) + share).astype(jnp.bfloat16)
        if s:
            carried = around(share, 1)
        block = following
    vmem = pl.BlockSpec(memory_space=pltpu.VMEM)
    return pl.pallas_call(
        blended_kernel,
        out_shape=jax.ShapeDtypeStruct(hidden.shape, jnp.bfloat16),
        in_specs=[vmem] * 4,
        out_specs=vmem,
        compiler_params=pltpu.CompilerParams(vmem_limit_bytes=8 * 2**20),
        name="blended",
    )(*in_vmem(hidden, own_share, carried, out_gain[None]))


def slot_layout(route_ids, experts, capacity):
    row_count, top_count = route_ids.shape
    flat_ids = route_ids.reshape(row_count * top_count)
    onehot = (flat_ids[:, None] == jnp.arange(experts, dtype=jnp.int32)[None, :]).astype(jnp.int32)
    before = jnp.cumsum(onehot, axis=0) - onehot
    slot_rank = jnp.sum(before * onehot, axis=1)
    position = flat_ids * capacity + slot_rank
    owners = jnp.arange(row_count * top_count, dtype=jnp.int32) // top_count
    slot_table = jnp.full((experts * capacity,), row_count, jnp.int32).at[position].set(owners)
    return (slot_table, position.reshape(row_count, top_count))


def routed_exchange(hidden, ids, weights, gate_local, up_local, down_local, out_gain, capacity):
    experts = lax.axis_size("sp")
    own_count, width = hidden.shape
    top_count = ids.shape[1]
    own_table, positions = slot_layout(ids, experts, capacity)
    padded = jnp.concatenate([hidden, jnp.zeros((1, width), jnp.bfloat16)], axis=0)
    dispatched = padded[own_table].reshape(experts, capacity, width)
    arrived = lax.all_to_all(dispatched, "sp", split_axis=0, concat_axis=0, tiled=True)
    gathered = lax.all_gather(arrived[None], "tp", axis=0, tiled=True)
    activity = expert_activity(gathered.reshape(-1, width), gate_local, up_local)
    expert_out = lax.psum_scatter(
        matmul(activity, down_local).astype(jnp.bfloat16), "tp", scatter_dimension=0, tiled=True
    )
    expert_out = expert_out.reshape(experts, capacity, width)
    returned = lax.all_to_all(expert_out, "sp", split_axis=0, concat_axis=0, tiled=True)
    picked = returned.reshape(experts * capacity, width)[positions.reshape(-1)]
    picked = picked.reshape(own_count, top_count, width)
    routed_sum = jnp.einsum("tk,tkd->td", weights, picked.astype(jnp.float32))
    return normalize(hidden.astype(jnp.float32) + routed_sum, out_gain).astype(jnp.bfloat16)


def shards(
    glu_value,
    glu_gate,
    conv_kernel,
    norm_gain,
    mix_weight,
    residual,
    resid_gain,
    expert_ids,
    route_weight,
    w_gate,
    w_up,
    w_down,
    out_gain,
):
    convolved, head, stats, gains = convolve(glu_value, glu_gate, conv_kernel, norm_gain)
    mixed_rows = scattered_product(convolved, head, stats, gains, mix_weight)
    vmem = pl.BlockSpec(memory_space=pltpu.VMEM)
    hidden = pl.pallas_call(
        hidden_kernel,
        out_shape=jax.ShapeDtypeStruct(residual.shape, jnp.bfloat16),
        in_specs=[vmem] * 5,
        out_specs=vmem,
        compiler_params=pltpu.CompilerParams(vmem_limit_bytes=8 * 2**20),
        name="hidden",
    )(residual, *mixed_rows, resid_gain[None])
    experts = lax.axis_size("sp")
    own_count, top_count = expert_ids.shape
    capacity = 2 * own_count * top_count // experts
    whole_rows = (experts // 2 - 1) * own_count + experts // 2 * capacity
    padded_rows = (experts - 1) * capacity
    ring = lax.axis_size("tp") == 4 and whole_rows <= 2 * padded_rows
    route = routed_ring if ring else routed_exchange
    return route(hidden, expert_ids, route_weight, w_gate[0], w_up[0], w_down[0], out_gain, capacity)


def solution(mesh):
    in_specs = (
        P("sp", "tp"),
        P("sp", "tp"),
        P(None, "tp"),
        P("tp"),
        P("tp", None),
        P(("sp", "tp"), None),
        P(),
        P(("sp", "tp"), None),
        P(("sp", "tp"), None),
        P("sp", None, "tp"),
        P("sp", None, "tp"),
        P("sp", "tp", None),
        P(),
    )
    out_specs = P(("sp", "tp"), None)
    return jax.shard_map(shards, mesh=mesh, in_specs=in_specs, out_specs=out_specs, check_vma=False)
```
